32 devices in a mesh: sp: 4 (over z), tp: 8 (over y, x, core).
Axes of the slice: x: 2, y: 2, z: 4, core: 2. Of those that a mesh axis runs over, the one named last changes fastest.
Arguments:
- tokens: bfloat16 [3072, 2048], P('sp'), may hold values from -6 to 6
- norm_gain: float32 [2048], replicated, may hold values from 0.5 to 80
- grid_query_weight: bfloat16 [2048, 2048], P(None, 'tp'), may hold values from -0.5 to 0.5
- grid_key_weight: bfloat16 [2048, 1024], P(None, 'tp'), may hold values from -0.5 to 0.5
- grid_value_weight: bfloat16 [2048, 1024], P(None, 'tp'), may hold values from -0.5 to 0.5
- grid_query_gain: float32 [128], replicated, may hold values from 1.6 to 6
- grid_key_gain: float32 [128], replicated, may hold values from 1.6 to 6
- local_query_weight: bfloat16 [2048, 2048], P(None, 'tp'), may hold values from -0.5 to 0.5
- local_key_weight: bfloat16 [2048, 1024], P(None, 'tp'), may hold values from -0.5 to 0.5
- local_value_weight: bfloat16 [2048, 1024], P(None, 'tp'), may hold values from -0.5 to 0.5
- sink_logit: float32 [16], P('tp'), may hold values from 1 to 6
- grid_out_weight: bfloat16 [2048, 2048], P('tp'), may hold values from -0.09375 to 0.09375
- local_out_weight: bfloat16 [2048, 2048], P('tp'), may hold values from -0.09375 to 0.09375
Outputs:
- mixed: bfloat16 [3072, 2048], P(('sp', 'tp'))
The draws below stay inside these ranges and needn't reach their ends.
All inputs are finite; a program needn't handle non-finite values.
Results may differ from the reference program's by a relative error of at most 0.03.
Values may be sent and summed in bfloat16 or wider, within the bound.
No kernel may reach another device: no remote copies, remote signals or barrier semaphores. Data moves between devices by JAX's collectives and lax.ppermute only.
A program may use at most 192 MiB of HBM per device.

```python
import jax
import jax.numpy as jnp
from jax import lax

D = 2048
HEAD = 128
GRID_HEADS = 16
GRID_KV = 8
LOCAL_HEADS = 16
LOCAL_KV = 8
WINDOW = 128
GRID_W = 64
SEQ = 3072
N_TP = 8


def shared_weight(key, salt, heads):
    drawn = jax.random.normal(jax.random.fold_in(key, salt), (D, heads * HEAD), jnp.float32) * D ** (-0.5)
    return jnp.clip(drawn, -0.5, 0.5)


def paired_key(key, salt, heads, groups):
    return shared_weight(key, salt + 1, groups)


def draw_grid_query_weight(key, part):
    return shared_weight(key, 101, GRID_HEADS).astype(jnp.bfloat16)


def draw_grid_key_weight(key, part):
    return paired_key(key, 101, GRID_HEADS, GRID_KV).astype(jnp.bfloat16)


def draw_local_query_weight(key, part):
    return shared_weight(key, 301, LOCAL_HEADS).astype(jnp.bfloat16)


def draw_local_key_weight(key, part):
    return paired_key(key, 301, LOCAL_HEADS, LOCAL_KV).astype(jnp.bfloat16)


def draw_norm_gain(key, part):
    base = jax.random.uniform(jax.random.fold_in(key, 201), (D,), jnp.float32, 0.5, 1.5)
    return base


def head_gain(key, salt):
    return jax.random.uniform(jax.random.fold_in(key, salt), (HEAD,), jnp.float32, 1.6, 2.4)


def draw_grid_query_gain(key, part):
    return head_gain(key, 401)


def draw_grid_key_gain(key, part):
    return head_gain(key, 402)


def level_of(key, dims, pieces, low, high):
    def one(dim, parts):
        draws = jax.random.uniform(jax.random.fold_in(jax.random.fold_in(key, 6), dim), (parts,), jnp.float32, low / len(pieces), high / len(pieces))
        return jnp.repeat(jnp.exp(draws), dims[dim] // parts).reshape((-1,) + (1,) * (len(dims) - dim - 1))

    level = one(*pieces[0])
    for cut in pieces[1:]:
        level = level * one(*cut)
    return level


def normal_values(key, dims, scale, reach, cuts=(), kind=jnp.bfloat16):
    entries = scale * jax.random.normal(key, dims, jnp.float32)
    if cuts:
        entries = entries * level_of(key, dims, cuts, -0.22, 0.18)
    return jnp.clip(entries, -reach, reach).astype(kind)


def setup_inputs(seed: int = 0) -> dict:
    key_list = jax.random.split(jax.random.key(seed), 14)
    return {
        "tokens": normal_values(key_list[0], (SEQ, D), 1.0, 6.0, ((0, 4),)),
        "norm_gain": draw_norm_gain(jax.random.fold_in(key_list[13], 71), 0),
        "grid_query_weight": draw_grid_query_weight(jax.random.fold_in(key_list[13], 71), 0),
        "grid_key_weight": draw_grid_key_weight(jax.random.fold_in(key_list[13], 71), 0),
        "grid_value_weight": normal_values(key_list[4], (D, GRID_KV * HEAD), (D // 16) ** -0.5, 0.5, ((1, 8),)),
        "grid_query_gain": draw_grid_query_gain(jax.random.fold_in(key_list[13], 71), 0),
        "grid_key_gain": draw_grid_key_gain(jax.random.fold_in(key_list[13], 71), 0),
        "local_query_weight": draw_local_query_weight(jax.random.fold_in(key_list[13], 71), 0),
        "local_key_weight": draw_local_key_weight(jax.random.fold_in(key_list[13], 71), 0),
        "local_value_weight": normal_values(key_list[9], (D, LOCAL_KV * HEAD), (D // 16) ** -0.5, 0.5, ((1, 8),)),
        "sink_logit": jnp.clip(1.0 + 5.0 * jax.random.uniform(key_list[10], (LOCAL_HEADS,), jnp.float32) ** level_of(key_list[10], (LOCAL_HEADS,), ((0, 8),), -0.2, 0.2), 1.0, 6.0),
        "grid_out_weight": normal_values(key_list[11], (GRID_HEADS * HEAD, D), (GRID_HEADS * HEAD + LOCAL_HEADS * HEAD) ** -0.5, 0.09375, ((0, 8),)),
        "local_out_weight": normal_values(key_list[12], (LOCAL_HEADS * HEAD, D), (GRID_HEADS * HEAD + LOCAL_HEADS * HEAD) ** -0.5, 0.09375, ((0, 8),)),
    }


EPSILON = 1e-06
ROPE_BASE = 10000.0

def rms_rows(values, gain):
    widened = values.astype(jnp.float32)
    return widened * lax.rsqrt(lax.optimization_barrier(jnp.mean(widened * widened, axis=-1, keepdims=True)) + EPSILON) * gain

def half_turn(part, angles):
    cosine = jnp.cos(angles)
    sine = jnp.sin(angles)
    cosine = jnp.concatenate([cosine, cosine], axis=-1)
    sine = jnp.concatenate([sine, sine], axis=-1)
    first, second = jnp.split(part, 2, axis=-1)
    turned = jnp.concatenate([-second, first], axis=-1)
    return part * cosine + turned * sine

def axial_turn(heads, positions):
    half_dim = heads.shape[-1] // 2
    inverse = ROPE_BASE ** (-jnp.arange(0, half_dim, 2, dtype=jnp.float32) / half_dim)
    row_angle = (positions // GRID_W).astype(jnp.float32)[:, None, None] * inverse
    col_angle = (positions % GRID_W).astype(jnp.float32)[:, None, None] * inverse
    return jnp.concatenate([half_turn(heads[..., :half_dim], row_angle), half_turn(heads[..., half_dim:], col_angle)], axis=-1)

def rounded_part(outs, weight, index, width):
    picked = lax.dynamic_slice_in_dim(outs, (index * width).astype(jnp.int32), width, 1)
    rows = lax.dynamic_slice_in_dim(weight, (index * width).astype(jnp.int32), width, 0)
    product = jnp.dot(picked, rows, preferred_element_type=jnp.float32).astype(jnp.bfloat16)
    return lax.optimization_barrier(product).astype(jnp.float32)

def reference(tokens, norm_gain, grid_query_weight, grid_key_weight, grid_value_weight, grid_query_gain, grid_key_gain, local_query_weight, local_key_weight, local_value_weight, sink_logit, grid_out_weight, local_out_weight):
    seq_len = tokens.shape[0]
    positions = jnp.arange(seq_len, dtype=jnp.int32)
    normed = rms_rows(tokens, norm_gain).astype(jnp.bfloat16)

    def project(weight):
        return jnp.dot(normed, weight, preferred_element_type=jnp.float32).astype(jnp.bfloat16)
    group_size = GRID_HEADS // GRID_KV
    score_scale = HEAD ** (-0.5)
    queries = axial_turn(rms_rows(project(grid_query_weight).reshape(seq_len, GRID_HEADS, HEAD), grid_query_gain), positions).astype(jnp.bfloat16).reshape(seq_len, GRID_KV, group_size, HEAD)
    keys = axial_turn(rms_rows(project(grid_key_weight).reshape(seq_len, GRID_KV, HEAD), grid_key_gain), positions).astype(jnp.bfloat16)
    values = project(grid_value_weight).reshape(seq_len, GRID_KV, HEAD)
    keys_wide = keys.astype(jnp.float32)
    values_wide = values.astype(jnp.float32)
    block_rows = min(512, seq_len)

    def one_block(start):
        block_q = lax.dynamic_slice_in_dim(queries, start, block_rows, 0).astype(jnp.float32)
        scores = jnp.einsum('qhgd,shd->hgqs', block_q, keys_wide) * score_scale
        weights = jax.nn.softmax(scores, axis=-1).astype(jnp.bfloat16)
        result = jnp.einsum('hgqs,shd->qhgd', weights.astype(jnp.float32), values_wide)
        return result.astype(jnp.bfloat16)
    starts = (jnp.arange(seq_len // block_rows) * block_rows).astype(jnp.int32)
    grid_out = lax.map(one_block, starts).reshape(seq_len, GRID_HEADS * HEAD)
    local_size = LOCAL_HEADS // LOCAL_KV
    blocks = seq_len // WINDOW
    local_q = project(local_query_weight).reshape(blocks, WINDOW, LOCAL_KV, local_size, HEAD)
    local_k = project(local_key_weight).reshape(seq_len, LOCAL_KV, HEAD)
    local_v = project(local_value_weight).reshape(seq_len, LOCAL_KV, HEAD)

    def banded(values_in):
        padded = jnp.pad(values_in, ((WINDOW, WINDOW), (0, 0), (0, 0))).reshape(blocks + 2, WINDOW, LOCAL_KV, HEAD)
        return jnp.concatenate([padded[:-2], padded[1:-1], padded[2:]], axis=1)
    band_k = banded(local_k).astype(jnp.float32)
    band_v = banded(local_v).astype(jnp.float32)
    scores = jnp.einsum('nqhgd,nshd->hgnqs', local_q.astype(jnp.float32), band_k) * score_scale
    relative = jnp.arange(3 * WINDOW)[None, :] - WINDOW - jnp.arange(WINDOW)[:, None]
    key_pos = jnp.arange(blocks)[:, None] * WINDOW - WINDOW + jnp.arange(3 * WINDOW)[None, :]
    valid = (jnp.abs(relative) <= WINDOW)[None] & ((key_pos >= 0) & (key_pos < seq_len))[:, None, :]
    scores = jnp.where(valid, scores, -jnp.inf)
    sink = sink_logit.reshape(LOCAL_KV, local_size, 1, 1, 1)
    top = jnp.maximum(lax.optimization_barrier(jnp.max(scores, axis=-1, keepdims=True)), sink)
    lifted = jnp.exp(scores - top)
    weights = (lifted / (lax.optimization_barrier(jnp.sum(lifted, axis=-1, keepdims=True)) + jnp.exp(sink - top))).astype(jnp.bfloat16)
    local_out = jnp.einsum('hgnqs,nshd->nqhgd', weights.astype(jnp.float32), band_v)
    local_out = local_out.astype(jnp.bfloat16).reshape(seq_len, LOCAL_HEADS * HEAD)
    grid_width = GRID_HEADS * HEAD // N_TP
    local_width = LOCAL_HEADS * HEAD // N_TP

    def add_group(index, total):
        total = total + rounded_part(grid_out, grid_out_weight, index, grid_width)
        return total + rounded_part(local_out, local_out_weight, index, local_width)
    total = lax.fori_loop(0, N_TP, add_group, jnp.zeros((seq_len, D), jnp.float32))
    return total.astype(jnp.bfloat16)
```

```python
import functools
import math

import jax
import jax.numpy as jnp
import numpy as np
from jax import lax
from jax.experimental import pallas as pl
from jax.experimental.pallas import tpu as pltpu
from jax.sharding import PartitionSpec as P

HEAD = 128
WINDOW = 128
GRID_W = 64
EPSILON = 1e-06
ROPE_BASE = 10000.0
MASKED = -1e30
MIB = 1 << 20

bf16 = jnp.bfloat16
f32 = jnp.float32
ROWS_T = (((1,), (1,)), ((), ()))


def dot(a, b):
    return jnp.dot(a, b, preferred_element_type=f32)


def turn_tables(total_rows, seq_devices):
    half = HEAD // 2
    quarter = half // 2
    inverse = (ROPE_BASE ** (-np.arange(0, half, 2, dtype=np.float32) / np.float32(half))).astype(np.float32)

    def tables(count, first):
        angles = np.arange(count, dtype=np.float32)[:, None] * inverse
        out = np.zeros((3, count, HEAD), np.float32)
        base = 0 if first else half
        out[0, :, base : base + quarter] = np.cos(angles)
        out[0, :, base + quarter : base + half] = np.cos(angles)
        out[1, :, base : base + quarter] = -np.sin(angles)
        out[2, :, base + quarter : base + half] = np.sin(angles)
        return out

    rows = tables(total_rows // GRID_W, True)
    rows = rows.reshape(3, seq_devices, -1, HEAD).transpose(1, 0, 2, 3)
    return rows, tables(GRID_W, False)


def norm_turn(part, gain, row_tab, col_tab, first_row, grid_rows):
    x = part.astype(bf16).astype(f32)
    x = x * lax.rsqrt(jnp.mean(x * x, axis=-1, keepdims=True) + EPSILON) * gain

    def table(k):
        rows = row_tab[k, pl.ds(first_row, grid_rows), :]
        return (rows[:, None, :] + col_tab[k][None, :, :]).reshape(grid_rows * GRID_W, HEAD)

    quarter = HEAD // 4
    return (
        x * table(0)
        + pltpu.roll(x, HEAD - quarter, 1) * table(1)
        + pltpu.roll(x, quarter, 1) * table(2)
    )


def kv_body(tile, steps, tok, gain, wk, wv, lwk, lwv, kgain, row_tab, col_tab, normed, up, down, lkv):
    step = pl.program_id(0)
    x = tok[...].astype(f32)
    n = (x * lax.rsqrt(jnp.mean(x * x, axis=-1, keepdims=True) + EPSILON) * gain[...]).astype(bf16)
    normed[...] = n
    y = dot(n, jnp.concatenate([wk[...], wv[...], lwk[...], lwv[...]], axis=1))
    grid_rows = tile // GRID_W
    keys = norm_turn(y[:, :HEAD], kgain[...], row_tab, col_tab, step * grid_rows, grid_rows)
    pair = jnp.concatenate([keys, y[:, HEAD : 2 * HEAD]], axis=1).astype(bf16)
    local = y[:, 2 * HEAD :].astype(bf16)
    rows = pl.ds(step * tile, tile)
    up[rows, :] = pair
    down[rows, :] = pair
    lkv[rows, :] = local

    @pl.when(step == steps - 1)
    def _():
        up[pl.ds(steps * tile, WINDOW), :] = local[tile - WINDOW :]

    @pl.when(step == 0)
    def _():
        down[pl.ds(steps * tile, WINDOW), :] = local[:WINDOW]


def q_body(tile, steps, normed, wq, lwq, qgain, row_tab, col_tab, q, lq):
    weights = jnp.concatenate([wq[...], lwq[...]], axis=1)
    heads = wq.shape[1] // HEAD
    grid_rows = tile // GRID_W
    for step in range(steps):
        rows = pl.ds(step * tile, tile)
        y = dot(normed[rows, :], weights)
        for h in range(heads):
            part = y[:, h * HEAD : (h + 1) * HEAD]
            turned = norm_turn(part, qgain[...], row_tab, col_tab, step * grid_rows, grid_rows)
            q[pl.ds(h * steps * tile + step * tile, tile), :] = turned.astype(bf16)
        lq[rows, :] = y[:, heads * HEAD :].astype(bf16)


def local_body(blocks, total_rows, info, sink, lq, lkv, low, high, out):
    offset = info[0] * (blocks * WINDOW)
    scale = HEAD ** (-0.5)
    row = lax.broadcasted_iota(jnp.int32, (WINDOW, 3 * WINDOW), 0)
    col = lax.broadcasted_iota(jnp.int32, (WINDOW, 3 * WINDOW), 1)
    band = jnp.abs(col - WINDOW - row) <= WINDOW
    pieces = [low[...]] + [lkv[pl.ds(i * WINDOW, WINDOW), :] for i in range(blocks)] + [high[...]]
    heads = lq.shape[1] // HEAD
    for i in range(blocks):
        keys = jnp.concatenate([p[:, :HEAD] for p in pieces[i : i + 3]], axis=0)
        values = jnp.concatenate([p[:, HEAD:] for p in pieces[i : i + 3]], axis=0)
        valid = band
        if i == 0 or i == blocks - 1:
            pos = offset + (i - 1) * WINDOW + col
            valid = band & (pos >= 0) & (pos < total_rows)
        for h in range(heads):
            query = lq[pl.ds(i * WINDOW, WINDOW), h * HEAD : (h + 1) * HEAD]
            s = lax.dot_general(query, keys, ROWS_T, preferred_element_type=f32) * scale
            s = jnp.where(valid, s, MASKED)
            top = jnp.maximum(jnp.max(s, axis=-1, keepdims=True), sink[0, h])
            p = jnp.exp(s - top)
            den = jnp.sum(p, axis=-1, keepdims=True) + jnp.exp(sink[0, h] - top)
            o = dot(p.astype(bf16), values) / den
            out[pl.ds(i * WINDOW, WINDOW), h * HEAD : (h + 1) * HEAD] = o.astype(bf16)


def attend_body(tile, spans, first, last, *refs):
    q = refs[0]
    kvs = refs[1 : 1 + len(spans)]
    rest = refs[1 + len(spans) :]
    if not first:
        m_in, acc_in, rest = rest[0], rest[1], rest[2:]
    rows_all = q.shape[0]
    ones = [jnp.ones((span, HEAD), bf16) for span in spans]
    for t in range(rows_all // tile):
        rows = pl.ds(t * tile, tile)
        query = q[rows, :]
        m = None if first else m_in[rows, :]
        acc = None if first else acc_in[rows, :]
        for kv, span, one in zip(kvs, spans, ones):
            keys = kv[pl.ds(0, span), :HEAD]
            values = jnp.concatenate([kv[pl.ds(0, span), HEAD:], one], axis=1)
            s = lax.dot_general(query, keys, ROWS_T, preferred_element_type=f32)
            top = jnp.broadcast_to(jnp.max(s, axis=-1, keepdims=True), (tile, HEAD))
            new = top if m is None else jnp.maximum(m, top)
            p = jnp.exp2(s - jnp.concatenate([new] * (span // HEAD), axis=1)).astype(bf16)
            add = dot(p, values)
            if m is None:
                acc = add
            else:
                factor = jnp.exp2(m - new)
                acc = acc * jnp.concatenate([factor, factor], axis=1) + add
            m = new
        if last:
            o = (acc[:, :HEAD] / acc[:, HEAD:]).astype(bf16)
            row_count = rest[0].shape[0]
            h, r = divmod(t * tile, row_count)
            rest[0][pl.ds(r, tile), h * HEAD : (h + 1) * HEAD] = o
        else:
            rest[0][rows, :] = m
            rest[1][rows, :] = acc


def vmem(count):
    return [pl.BlockSpec(memory_space=pltpu.VMEM)] * count


def sds(shape, dtype):
    return jax.ShapeDtypeStruct(shape, dtype)


def cost(flops, transcendentals=0, bytes_accessed=0):
    return pl.CostEstimate(flops=int(flops), transcendentals=int(transcendentals), bytes_accessed=int(bytes_accessed))


def attend(q, blocks, state, last, row_count):
    rows, tile = q.shape[0], 256
    spans = tuple(b[1] for b in blocks)
    operands = [q] + [b[0] for b in blocks] + ([] if state is None else list(state))
    if last:
        shape = sds((row_count, rows // row_count * HEAD), bf16)
    else:
        shape = (sds((rows, HEAD), f32), sds((rows, 2 * HEAD), f32))
    keys = sum(spans)
    return pl.pallas_call(
        functools.partial(attend_body, tile, spans, state is None, last),
        out_shape=shape,
        in_specs=vmem(len(operands)),
        out_specs=pl.BlockSpec(memory_space=pltpu.VMEM) if last else tuple(vmem(2)),
        compiler_params=pltpu.CompilerParams(vmem_limit_bytes=24 * MIB),
        cost_estimate=cost(rows * keys * HEAD * 8, rows * keys),
        name="attend",
    )(*operands)


def shards(
    tokens,
    norm_gain,
    grid_query_weight,
    grid_key_weight,
    grid_value_weight,
    grid_query_gain,
    grid_key_gain,
    local_query_weight,
    local_key_weight,
    local_value_weight,
    sink_logit,
    grid_out_weight,
    local_out_weight,
):
    row_count, width = tokens.shape
    n_sp = lax.axis_size("sp")
    n_tp = lax.axis_size("tp")
    total_rows = row_count * n_sp
    sp = lax.axis_index("sp")
    tp = lax.axis_index("tp")
    heads = grid_query_weight.shape[1] // HEAD
    row_np, col_np = turn_tables(total_rows, n_sp)
    row_tab = lax.dynamic_index_in_dim(jnp.asarray(row_np), sp, 0, keepdims=False)
    col_tab = jnp.asarray(col_np)

    tile = 256
    steps = row_count // tile
    fixed = lambda *shape: pl.BlockSpec(shape, lambda i: (0,) * len(shape))
    grid_rows = row_count // GRID_W
    normed, up, down, lkv = pl.pallas_call(
        functools.partial(kv_body, tile, steps),
        grid=(steps,),
        out_shape=(
            sds((row_count, width), bf16),
            sds((row_count + WINDOW, 2 * HEAD), bf16),
            sds((row_count + WINDOW, 2 * HEAD), bf16),
            sds((row_count, 2 * HEAD), bf16),
        ),
        in_specs=[
            pl.BlockSpec((tile, width), lambda i: (i, 0)),
            fixed(1, width),
            fixed(width, HEAD),
            fixed(width, HEAD),
            fixed(width, HEAD),
            fixed(width, HEAD),
            fixed(1, HEAD),
            fixed(3, grid_rows, HEAD),
            fixed(3, GRID_W, HEAD),
        ],
        out_specs=(
            pl.BlockSpec((tile, width), lambda i: (i, 0)),
            fixed(row_count + WINDOW, 2 * HEAD),
            fixed(row_count + WINDOW, 2 * HEAD),
            fixed(row_count, 2 * HEAD),
        ),
        compiler_params=pltpu.CompilerParams(vmem_limit_bytes=24 * MIB),
        cost_estimate=cost(2 * row_count * width * 4 * HEAD, 0, 8 * MIB),
        name="keys",
    )(
        tokens,
        norm_gain.reshape(1, width),
        grid_key_weight,
        grid_value_weight,
        local_key_weight,
        local_value_weight,
        grid_key_gain.reshape(1, HEAD),
        row_tab,
        col_tab,
    )

    forward = [(i, (i + 1) % n_sp) for i in range(n_sp)]
    backward = [(t, s) for s, t in forward]
    from_low = lax.ppermute(up, "sp", forward)
    from_high = lax.ppermute(down, "sp", backward)

    fold = HEAD ** (-0.5) * math.log2(math.e)
    q, lq = pl.pallas_call(
        functools.partial(q_body, tile, steps),
        out_shape=(sds((heads * row_count, HEAD), bf16), sds((row_count, heads * HEAD), bf16)),
        in_specs=vmem(6),
        out_specs=tuple(vmem(2)),
        compiler_params=pltpu.CompilerParams(vmem_limit_bytes=24 * MIB),
        cost_estimate=cost(2 * row_count * width * 4 * HEAD, 0, 6 * MIB),
        name="queries",
    )(normed, grid_query_weight, local_query_weight, (grid_query_gain * fold).reshape(1, HEAD), row_tab, col_tab)

    state = attend(q, [(up, row_count)], None, False, row_count)

    low, high = from_low, from_high
    pending = []
    for _ in range(1, (n_sp - 1) // 2):
        next_low = lax.ppermute(low[:row_count], "sp", forward)
        next_high = lax.ppermute(high[:row_count], "sp", backward)
        state = attend(q, [(low, row_count), (high, row_count)], state, False, row_count)
        low, high = next_low, next_high
    half = row_count // 2
    far_low = lax.ppermute(low[:half], "sp", forward)
    far_high = lax.ppermute(high[half:row_count], "sp", backward)

    local_out = pl.pallas_call(
        functools.partial(local_body, row_count // WINDOW, total_rows),
        out_shape=sds((row_count, heads * HEAD), bf16),
        in_specs=[pl.BlockSpec(memory_space=pltpu.SMEM)] * 2 + vmem(4),
        out_specs=pl.BlockSpec(memory_space=pltpu.VMEM),
        compiler_params=pltpu.CompilerParams(vmem_limit_bytes=24 * MIB),
        cost_estimate=cost(heads * row_count * 3 * WINDOW * HEAD * 8, heads * row_count * 3 * WINDOW),
        name="banded",
    )(
        sp.reshape(1).astype(jnp.int32),
        sink_logit.reshape(1, heads),
        lq,
        lkv,
        lax.slice_in_dim(from_low, row_count, row_count + WINDOW),
        lax.slice_in_dim(from_high, row_count, row_count + WINDOW),
    )
    state = attend(q, [(low, row_count), (high, row_count)], state, False, row_count)
    grid_out = attend(q, [(far_low, half), (far_high, half)], state, True, row_count)

    flip = lambda bit: [(i, i ^ bit) for i in range(n_tp)]
    take = lambda v, i, axis: lax.dynamic_index_in_dim(v, i, axis, keepdims=False)
    b0, b1, b2 = tp % 2, (tp // 2) % 2, tp // 4
    piece = row_count // n_tp
    both = jnp.concatenate([grid_out, local_out], axis=1)
    weights = jnp.concatenate([grid_out_weight, local_out_weight], axis=0)
    partial = dot(both, weights).reshape(2, 2, 2, piece, width)
    got = lax.ppermute(take(partial, 1 - b0, 2).astype(bf16), "tp", flip(1))
    acc = take(partial, b0, 2) + got.astype(f32)
    side = width // 2
    left, right = acc[..., :side], acc[..., side:]
    got_l = lax.ppermute(take(left, 1 - b1, 1).astype(bf16), "tp", flip(2))
    got_r = lax.ppermute(take(right, 1 - b2, 0).astype(bf16), "tp", flip(4))
    left = take(left, b1, 1) + got_l.astype(f32)
    right = take(right, b2, 0) + got_r.astype(f32)
    got_l = lax.ppermute(take(left, 1 - b2, 0).astype(bf16), "tp", flip(4))
    got_r = lax.ppermute(take(right, 1 - b1, 0).astype(bf16), "tp", flip(2))
    left = take(left, b2, 0) + got_l.astype(f32)
    right = take(right, b1, 0) + got_r.astype(f32)
    return jnp.concatenate([left, right], axis=1).astype(bf16)


def solution(mesh):
    in_specs = (
        P("sp", None),
        P(),
        P(None, "tp"),
        P(None, "tp"),
        P(None, "tp"),
        P(),
        P(),
        P(None, "tp"),
        P(None, "tp"),
        P(None, "tp"),
        P("tp"),
        P("tp", None),
        P("tp", None),
    )
    out_specs = P(("sp", "tp"), None)
    return jax.shard_map(shards, mesh=mesh, in_specs=in_specs, out_specs=out_specs, check_vma=False)
```

```python
import functools
import math

import jax
import jax.numpy as jnp
import numpy as np
from jax import lax
from jax.experimental import pallas as pl
from jax.experimental.pallas import tpu as pltpu
from jax.sharding import PartitionSpec as P

HEAD = 128
WINDOW = 128
GRID_W = 64
EPSILON = 1e-06
ROPE_BASE = 10000.0
MASKED = -1e30
MIB = 1 << 20

bf16 = jnp.bfloat16
f32 = jnp.float32
ROWS_T = (((1,), (1,)), ((), ()))


def dot(a, b):
    return jnp.dot(a, b, preferred_element_type=f32)


def turn_tables(total_rows, seq_devices):
    half = HEAD // 2
    quarter = half // 2
    inverse = (ROPE_BASE ** (-np.arange(0, half, 2, dtype=np.float32) / np.float32(half))).astype(np.float32)

    def tables(count, first):
        angles = np.arange(count, dtype=np.float32)[:, None] * inverse
        out = np.zeros((3, count, HEAD), np.float32)
        base = 0 if first else half
        out[0, :, base : base + quarter] = np.cos(angles)
        out[0, :, base + quarter : base + half] = np.cos(angles)
        out[1, :, base : base + quarter] = -np.sin(angles)
        out[2, :, base + quarter : base + half] = np.sin(angles)
        return out

    rows = tables(total_rows // GRID_W, True)
    rows = rows.reshape(3, seq_devices, -1, HEAD).transpose(1, 0, 2, 3)
    return rows, tables(GRID_W, False)


def norm_turn(part, gain, row_tab, col_tab, first_row, grid_rows):
    x = part.astype(bf16).astype(f32)
    x = x * lax.rsqrt(jnp.mean(x * x, axis=-1, keepdims=True) + EPSILON) * gain

    def table(k):
        rows = row_tab[k, pl.ds(first_row, grid_rows), :]
        return (rows[:, None, :] + col_tab[k][None, :, :]).reshape(grid_rows * GRID_W, HEAD)

    quarter = HEAD // 4
    return (
        x * table(0)
        + pltpu.roll(x, HEAD - quarter, 1) * table(1)
        + pltpu.roll(x, quarter, 1) * table(2)
    )


def start_copies(pairs, sems):
    copies = [pltpu.make_async_copy(src, dst, sems.at[i]) for i, (src, dst) in enumerate(pairs)]
    for copy in copies:
        copy.start()
    return copies


def kv_body(tile, steps, info, tok, gain, wk, wv, lwk, lwv, kgain, row_tab, col_tab,
            normed, kv, lkv, first_edge, last_edge,
            tok_v, gain_v, w_v, kgain_v, row_v, col_v, sems):
    rows = [pl.ds(i * tile, tile) for i in range(steps)]
    pairs = [(gain, gain_v), (tok.at[rows[0]], tok_v.at[rows[0]])]
    pairs += [(w, w_v.at[i]) for i, w in enumerate((wk, wv, lwk, lwv))]
    pairs += [(kgain, kgain_v), (row_tab.at[info[0]], row_v), (col_tab, col_v)]
    fixed = len(pairs)
    pairs += [(tok.at[r], tok_v.at[r]) for r in rows[1:]]
    copies = start_copies(pairs, sems)
    copies[0].wait()
    grid_rows = tile // GRID_W
    for i, r in enumerate(rows):
        copies[1 if i == 0 else fixed + i - 1].wait()
        x = tok_v[r, :].astype(f32)
        n = (x * lax.rsqrt(jnp.mean(x * x, axis=-1, keepdims=True) + EPSILON) * gain_v[...]).astype(bf16)
        normed[r, :] = n
        if i == 0:
            for copy in copies[2:fixed]:
                copy.wait()
        y = dot(n, jnp.concatenate([w_v[k] for k in range(4)], axis=1))
        keys = norm_turn(y[:, :HEAD], kgain_v[...], row_v, col_v, i * grid_rows, grid_rows)
        kv[r, :] = jnp.concatenate([keys, y[:, HEAD : 2 * HEAD]], axis=1).astype(bf16)
        lkv[r, :] = y[:, 2 * HEAD :].astype(bf16)
    first_edge[...] = lkv[pl.ds(0, WINDOW), :]
    last_edge[...] = lkv[pl.ds(steps * tile - WINDOW, WINDOW), :]


def q_body(tile, steps, info, normed, wq, lwq, qgain, row_tab, col_tab, q, lq, wq_v, lwq_v, row_v, col_v, sems):
    copies = start_copies([(wq, wq_v), (lwq, lwq_v), (row_tab.at[info[0]], row_v), (col_tab, col_v)], sems)
    for copy in copies:
        copy.wait()
    heads = wq.shape[1] // HEAD
    grid_rows = tile // GRID_W
    for step in range(steps):
        rows = pl.ds(step * tile, tile)
        y = dot(normed[rows, :], jnp.concatenate([wq_v[...], lwq_v[...]], axis=1))
        for h in range(heads):
            part = y[:, h * HEAD : (h + 1) * HEAD]
            turned = norm_turn(part, qgain[...], row_v, col_v, step * grid_rows, grid_rows)
            q[pl.ds(h * steps * tile + step * tile, tile), :] = turned.astype(bf16)
        lq[rows, :] = y[:, heads * HEAD :].astype(bf16)


def split_rows(info, whole, keep, send):
    piece = keep.shape[0] // (whole.shape[0] // keep.shape[0] * 2)
    count = keep.shape[0] // piece
    for part, flip in ((keep, 0), (send, 1)):
        for i in range(count):
            start = pl.multiple_of(2 * i * piece + (info[1] ^ flip) * piece, 16)
            part[pl.ds(i * piece, piece), :] = whole[pl.ds(start, piece), :]


def local_body(blocks, total_rows, info, sink, lq, lkv, low, high, after_low, after_high, keep, send, out):
    offset = info[0] * (blocks * WINDOW)
    scale = HEAD ** (-0.5)
    row = lax.broadcasted_iota(jnp.int32, (WINDOW, 3 * WINDOW), 0)
    col = lax.broadcasted_iota(jnp.int32, (WINDOW, 3 * WINDOW), 1)
    band = jnp.abs(col - WINDOW - row) <= WINDOW
    pieces = [low[...]] + [lkv[pl.ds(i * WINDOW, WINDOW), :] for i in range(blocks)] + [high[...]]
    heads = lq.shape[1] // HEAD
    for i in range(blocks):
        keys = jnp.concatenate([p[:, :HEAD] for p in pieces[i : i + 3]], axis=0)
        values = jnp.concatenate([p[:, HEAD:] for p in pieces[i : i + 3]], axis=0)
        valid = band
        if i == 0 or i == blocks - 1:
            pos = offset + (i - 1) * WINDOW + col
            valid = band & (pos >= 0) & (pos < total_rows)
        for h in range(heads):
            query = lq[pl.ds(i * WINDOW, WINDOW), h * HEAD : (h + 1) * HEAD]
            s = lax.dot_general(query, keys, ROWS_T, preferred_element_type=f32) * scale
            s = jnp.where(valid, s, MASKED)
            top = jnp.maximum(jnp.max(s, axis=-1, keepdims=True), sink[0, h])
            p = jnp.exp(s - top)
            den = jnp.sum(p, axis=-1, keepdims=True) + jnp.exp(sink[0, h] - top)
            o = dot(p.astype(bf16), values) / den
            out[pl.ds(i * WINDOW, WINDOW), h * HEAD : (h + 1) * HEAD] = o.astype(bf16)
    split_rows(info, out, keep, send)


def attend_body(tile, spans, first, last, *refs):
    info, q = refs[:2]
    kvs = refs[2 : 2 + len(spans)]
    rest = refs[2 + len(spans) :]
    if not first:
        m_in, acc_in, rest = rest[0], rest[1], rest[2:]
    rows_all = q.shape[0]
    ones = [jnp.ones((span, HEAD), bf16) for span in spans]
    for t in range(rows_all // tile):
        rows = pl.ds(t * tile, tile)
        query = q[rows, :]
        m = None if first else m_in[rows, :]
        acc = None if first else acc_in[rows, :]
        for kv, span, one in zip(kvs, spans, ones):
            keys = kv[pl.ds(0, span), :HEAD]
            values = jnp.concatenate([kv[pl.ds(0, span), HEAD:], one], axis=1)
            s = lax.dot_general(query, keys, ROWS_T, preferred_element_type=f32)
            top = jnp.broadcast_to(jnp.max(s, axis=-1, keepdims=True), (tile, HEAD))
            new = top if m is None else jnp.maximum(m, top)
            p = jnp.exp2(s - jnp.concatenate([new] * (span // HEAD), axis=1)).astype(bf16)
            add = dot(p, values)
            if m is None:
                acc = add
            else:
                factor = jnp.exp2(m - new)
                acc = acc * jnp.concatenate([factor, factor], axis=1) + add
            m = new
        if last:
            o = (acc[:, :HEAD] / acc[:, HEAD:]).astype(bf16)
            whole = rest[2]
            h, r = divmod(t * tile, whole.shape[0])
            whole[pl.ds(r, tile), h * HEAD : (h + 1) * HEAD] = o
        else:
            rest[0][rows, :] = m
            rest[1][rows, :] = acc
    if last:
        split_rows(info, rest[2], rest[0], rest[1])


def project_body(count, slots, info, keep, other, lkeep, lother, w, lw, w_other, lw_other, *outs):
    piece = outs[0].shape[-2]
    weights = jnp.concatenate([w[...], w_other[...], lw[...], lw_other[...]], axis=0)
    for slot, out in zip(slots, outs):
        rows = pl.ds(pl.multiple_of(info[slot] * piece, 16), piece)
        part = jnp.concatenate([ref[rows, :] for ref in (keep, other, lkeep, lother)], axis=1)
        out[...] = dot(part, weights).astype(out.dtype)


def vmem(count):
    return [pl.BlockSpec(memory_space=pltpu.VMEM)] * count


def sds(shape, dtype):
    return jax.ShapeDtypeStruct(shape, dtype)


def cost(flops, transcendentals=0, bytes_accessed=0):
    return pl.CostEstimate(flops=int(flops), transcendentals=int(transcendentals), bytes_accessed=int(bytes_accessed))


def hbm(count):
    return [pl.BlockSpec(memory_space=pltpu.HBM)] * count


SCALARS = [pl.BlockSpec(memory_space=pltpu.SMEM)]


def in_hbm(*arrays):
    return [pltpu.with_memory_space_constraint(a, pltpu.HBM) for a in arrays]


def params(mib):
    return pltpu.CompilerParams(vmem_limit_bytes=mib * MIB)


def attend(info, q, blocks, state, last, row_count):
    rows, tile = q.shape[0], 256
    spans = tuple(b[1] for b in blocks)
    operands = [q] + [b[0] for b in blocks] + ([] if state is None else list(state))
    lanes = rows // row_count * HEAD
    if last:
        shape = (sds((row_count // 2, lanes), bf16),) * 2
    else:
        shape = (sds((rows, HEAD), f32), sds((rows, 2 * HEAD), f32))
    keys = sum(spans)
    return pl.pallas_call(
        functools.partial(attend_body, tile, spans, state is None, last),
        out_shape=shape,
        in_specs=SCALARS + vmem(len(operands)),
        out_specs=tuple(vmem(2)),
        scratch_shapes=[pltpu.VMEM((row_count, lanes), bf16)] if last else [],
        compiler_params=params(16),
        cost_estimate=cost(rows * keys * HEAD * 8, rows * keys),
        name="attend",
    )(info, *operands)


def project(info, slots, operands, piece, dtype):
    width = operands[-1].shape[1]
    depth = 4 * operands[0].shape[1]
    return pl.pallas_call(
        functools.partial(project_body, len(slots), slots),
        out_shape=tuple(sds((piece, width), dtype) for _ in slots),
        in_specs=SCALARS + vmem(8),
        out_specs=tuple(vmem(len(slots))),
        compiler_params=params(8),
        cost_estimate=cost(2 * piece * width * depth * len(slots), 0, 4 * MIB),
        name="project",
    )(info, *operands)


def shards(
    tokens,
    norm_gain,
    grid_query_weight,
    grid_key_weight,
    grid_value_weight,
    grid_query_gain,
    grid_key_gain,
    local_query_weight,
    local_key_weight,
    local_value_weight,
    sink_logit,
    grid_out_weight,
    local_out_weight,
):
    row_count, width = tokens.shape
    n_sp = lax.axis_size("sp")
    n_tp = lax.axis_size("tp")
    total_rows = row_count * n_sp
    sp = lax.axis_index("sp")
    tp = lax.axis_index("tp")
    heads = grid_query_weight.shape[1] // HEAD
    row_np, col_np = turn_tables(total_rows, n_sp)
    row_tab, col_tab = jnp.asarray(row_np), jnp.asarray(col_np)

    core, mine = tp % 2, tp // 2
    near, far = 1 + core, 2 - core
    info = jnp.stack([sp, core, mine ^ 3, mine ^ near, mine ^ far, mine]).astype(jnp.int32)

    tile = 128
    steps = row_count // tile
    table_shape = (3, row_count // GRID_W, HEAD)
    normed, kv, lkv, first_edge, last_edge = pl.pallas_call(
        functools.partial(kv_body, tile, steps),
        out_shape=(
            sds((row_count, width), bf16),
            sds((row_count, 2 * HEAD), bf16),
            sds((row_count, 2 * HEAD), bf16),
            sds((WINDOW, 2 * HEAD), bf16),
            sds((WINDOW, 2 * HEAD), bf16),
        ),
        in_specs=SCALARS + hbm(9),
        out_specs=tuple(vmem(5)),
        scratch_shapes=[
            pltpu.VMEM((row_count, width), bf16),
            pltpu.VMEM((1, width), f32),
            pltpu.VMEM((4, width, HEAD), bf16),
            pltpu.VMEM((1, HEAD), f32),
            pltpu.VMEM(table_shape, f32),
            pltpu.VMEM((3, GRID_W, HEAD), f32),
            pltpu.SemaphoreType.DMA((9 + steps - 1,)),
        ],
        compiler_params=params(24),
        cost_estimate=cost(2 * row_count * width * 4 * HEAD, 0, 8 * MIB),
        name="keys",
    )(
        info,
        *in_hbm(
            tokens,
            norm_gain.reshape(1, width),
            grid_key_weight,
            grid_value_weight,
            local_key_weight,
            local_value_weight,
            grid_key_gain.reshape(1, HEAD),
            row_tab,
            col_tab,
        ),
    )

    forward = [(i, (i + 1) % n_sp) for i in range(n_sp)]
    backward = [(t, s) for s, t in forward]
    low = lax.ppermute(kv, "sp", forward)
    high = lax.ppermute(kv, "sp", backward)
    low_edge = lax.ppermute(last_edge, "sp", forward[:-1])
    high_edge = lax.ppermute(first_edge, "sp", backward[:-1])

    fold = HEAD ** (-0.5) * math.log2(math.e)
    q, lq = pl.pallas_call(
        functools.partial(q_body, 256, row_count // 256),
        out_shape=(sds((heads * row_count, HEAD), bf16), sds((row_count, heads * HEAD), bf16)),
        in_specs=SCALARS + vmem(1) + hbm(2) + vmem(1) + hbm(2),
        out_specs=tuple(vmem(2)),
        scratch_shapes=[
            pltpu.VMEM((width, heads * HEAD), bf16),
            pltpu.VMEM((width, heads * HEAD), bf16),
            pltpu.VMEM(table_shape, f32),
            pltpu.VMEM((3, GRID_W, HEAD), f32),
            pltpu.SemaphoreType.DMA((4,)),
        ],
        compiler_params=params(24),
        cost_estimate=cost(2 * row_count * width * 4 * HEAD, 0, 6 * MIB),
        name="queries",
    )(
        info,
        normed,
        *in_hbm(grid_query_weight, local_query_weight),
        (grid_query_gain * fold).reshape(1, HEAD),
        *in_hbm(row_tab, col_tab),
    )

    flip = [(i, i ^ 1) for i in range(n_tp)]
    first_hop = [(i, i ^ (2 + 2 * (i % 2))) for i in range(n_tp)]
    second_hop = [(i, i ^ (4 - 2 * (i % 2))) for i in range(n_tp)]
    w_other = lax.ppermute(grid_out_weight, "tp", flip)
    lw_other = lax.ppermute(local_out_weight, "tp", flip)

    state = attend(info, q, [(kv, row_count)], None, False, row_count)
    for _ in range(1, (n_sp - 1) // 2):
        next_low = lax.ppermute(low, "sp", forward)
        next_high = lax.ppermute(high, "sp", backward)
        state = attend(info, q, [(low, row_count), (high, row_count)], state, False, row_count)
        low, high = next_low, next_high
    half = row_count // 2
    cut_low, cut_high = low[:half], high[half:]
    far_low = lax.ppermute(cut_low, "sp", forward)
    far_high = lax.ppermute(cut_high, "sp", backward)

    lkeep, lsend = pl.pallas_call(
        functools.partial(local_body, row_count // WINDOW, total_rows),
        out_shape=(sds((row_count // 2, heads * HEAD), bf16),) * 2,
        in_specs=SCALARS * 2 + vmem(6),
        out_specs=tuple(vmem(2)),
        scratch_shapes=[pltpu.VMEM((row_count, heads * HEAD), bf16)],
        compiler_params=params(16),
        cost_estimate=cost(heads * row_count * 3 * WINDOW * HEAD * 8, heads * row_count * 3 * WINDOW),
        name="banded",
    )(info, sink_logit.reshape(1, heads), lq, lkv, low_edge, high_edge, cut_low, cut_high)
    lother = lax.ppermute(lsend, "tp", flip)
    state = attend(info, q, [(low, row_count), (high, row_count)], state, False, row_count)
    keep, send = attend(info, q, [(far_low, half), (far_high, half)], state, True, row_count)
    other = lax.ppermute(send, "tp", flip)

    piece = row_count // n_tp
    operands = (keep, other, lkeep, lother, grid_out_weight, local_out_weight, w_other, lw_other)
    (pass_on,) = project(info, (2,), operands, piece, bf16)
    got_on = lax.ppermute(pass_on, "tp", first_hop)
    (direct,) = project(info, (3,), operands, piece, bf16)
    got = lax.ppermute(direct, "tp", first_hop)
    next_part, own_part = project(info, (4, 5), operands, piece, f32)
    got_next = lax.ppermute((next_part + got_on.astype(f32)).astype(bf16), "tp", second_hop)
    return (own_part + got.astype(f32) + got_next.astype(f32)).astype(bf16)


def solution(mesh):
    in_specs = (
        P("sp", None),
        P(),
        P(None, "tp"),
        P(None, "tp"),
        P(None, "tp"),
        P(),
        P(),
        P(None, "tp"),
        P(None, "tp"),
        P(None, "tp"),
        P("tp"),
        P("tp", None),
        P("tp", None),
    )
    out_specs = P(("sp", "tp"), None)
    return jax.shard_map(shards, mesh=mesh, in_specs=in_specs, out_specs=out_specs, check_vma=False)
```

```python
import functools
import math

import jax
import jax.numpy as jnp
import numpy as np
from jax import lax
from jax.experimental import pallas as pl
from jax.experimental.pallas import tpu as pltpu
from jax.sharding import PartitionSpec as P

HEAD = 128
WINDOW = 128
GRID_W = 64
EPSILON = 1e-06
ROPE_BASE = 10000.0
MASKED = -1e30
LOG2E = math.log2(math.e)
MIB = 1 << 20

bf16 = jnp.bfloat16
f32 = jnp.float32
ROWS_T = (((1,), (1,)), ((), ()))


def dot(a, b):
    return jnp.dot(a, b, preferred_element_type=f32)


def turn_tables(total_rows, seq_devices):
    half = HEAD // 2
    quarter = half // 2
    inverse = (ROPE_BASE ** (-np.arange(0, half, 2, dtype=np.float32) / np.float32(half))).astype(np.float32)

    def tables(count, first):
        angles = np.arange(count, dtype=np.float32)[:, None] * inverse
        out = np.zeros((3, count, HEAD), np.float32)
        base = 0 if first else half
        out[0, :, base : base + quarter] = np.cos(angles)
        out[0, :, base + quarter : base + half] = np.cos(angles)
        out[1, :, base : base + quarter] = -np.sin(angles)
        out[2, :, base + quarter : base + half] = np.sin(angles)
        return out

    rows = tables(total_rows // GRID_W, True)
    rows = rows.reshape(3, seq_devices, -1, HEAD).transpose(1, 0, 2, 3)
    return rows, tables(GRID_W, False)


def norm_turn(part, gain, row_tab, col_tab, first_row, grid_rows):
    x = part.astype(bf16).astype(f32)
    x = x * lax.rsqrt(jnp.mean(x * x, axis=-1, keepdims=True) + EPSILON) * gain

    def table(k):
        rows = row_tab[k, pl.ds(first_row, grid_rows), :]
        return (rows[:, None, :] + col_tab[k][None, :, :]).reshape(grid_rows * GRID_W, HEAD)

    quarter = HEAD // 4
    return (
        x * table(0)
        + pltpu.roll(x, HEAD - quarter, 1) * table(1)
        + pltpu.roll(x, quarter, 1) * table(2)
    )


def place():
    tp = lax.axis_index("tp")
    core, mine = tp % 2, tp // 2
    return lax.axis_index("sp"), core, (mine ^ 3, mine ^ (1 + core), mine ^ (2 - core), mine)


def start_copies(pairs, sems):
    copies = [pltpu.make_async_copy(src, dst, sems.at[i]) for i, (src, dst) in enumerate(pairs)]
    for copy in copies:
        copy.start()
    return copies


def kv_body(tile, tok, gain, wk, wv, kgain, row_tab, col_tab,
            normed, kv, tok_v, gain_v, wk_v, wv_v, kgain_v, row_v, col_v, sems):
    row_count = tok.shape[0]
    rows = [pl.ds(i, tile) for i in range(0, row_count, tile)]
    pairs = [(gain, gain_v)] + [(tok.at[r], tok_v.at[r]) for r in rows]
    pairs += [(wk, wk_v), (wv, wv_v), (kgain, kgain_v), (row_tab.at[place()[0]], row_v), (col_tab, col_v)]
    copies = start_copies(pairs, sems)
    copies[0].wait()
    for r, copy in zip(rows, copies[1:]):
        copy.wait()
        x = tok_v[r, :].astype(f32)
        normed[r, :] = (
            x * lax.rsqrt(jnp.mean(x * x, axis=-1, keepdims=True) + EPSILON) * gain_v[...]
        ).astype(bf16)
    for copy in copies[1 + len(rows) :]:
        copy.wait()
    y = dot(normed[...], jnp.concatenate([wk_v[...], wv_v[...]], axis=1))
    keys = norm_turn(y[:, :HEAD], kgain_v[...], row_v, col_v, 0, row_count // GRID_W)
    kv[...] = jnp.concatenate([keys, y[:, HEAD:]], axis=1).astype(bf16)


def q_body(tile, normed, wq, lwq, lwk, lwv, qgain, row_tab, col_tab,
           q, lq, lkv, first_edge, last_edge, wq_v, lwq_v, lwk_v, lwv_v, row_v, col_v, sems):
    pairs = [(lwq, lwq_v), (lwk, lwk_v), (lwv, lwv_v), (wq, wq_v), (row_tab.at[place()[0]], row_v), (col_tab, col_v)]
    copies = start_copies(pairs, sems)
    for copy in copies:
        copy.wait()
    row_count = normed.shape[0]
    heads = wq.shape[1] // HEAD
    grid_rows = tile // GRID_W
    for start in range(0, row_count, tile):
        rows = pl.ds(start, tile)
        y = dot(normed[rows, :], jnp.concatenate([wq_v[...], lwq_v[...], lwk_v[...], lwv_v[...]], axis=1))
        for h in range(heads):
            part = y[:, h * HEAD : (h + 1) * HEAD]
            turned = norm_turn(part, qgain[...], row_v, col_v, start // GRID_W, grid_rows)
            q[pl.ds(h * row_count + start, tile), :] = turned.astype(bf16)
        lq[rows, :] = y[:, heads * HEAD : 2 * heads * HEAD].astype(bf16)
        lkv[rows, :] = y[:, 2 * heads * HEAD :].astype(bf16)
    first_edge[...] = lkv[pl.ds(0, WINDOW), :]
    last_edge[...] = lkv[pl.ds(row_count - WINDOW, WINDOW), :]


def split_rows(whole, keep, send):
    piece = keep.shape[0] // (whole.shape[0] // keep.shape[0] * 2)
    count = keep.shape[0] // piece
    core = place()[1]
    for part, flip in ((keep, 0), (send, 1)):
        for i in range(count):
            start = pl.multiple_of(2 * i * piece + (core ^ flip) * piece, 16)
            part[pl.ds(i * piece, piece), :] = whole[pl.ds(start, piece), :]


def local_body(blocks, total_rows, sink, lq, lkv, low, high, after_low, after_high, keep, send, out):
    offset = place()[0] * (blocks * WINDOW)
    scale = HEAD ** (-0.5) * LOG2E
    heads = lq.shape[1] // HEAD
    shape = (heads * WINDOW, 3 * WINDOW)
    row = lax.broadcasted_iota(jnp.int32, shape, 0) % WINDOW
    col = lax.broadcasted_iota(jnp.int32, shape, 1)
    band = jnp.abs(col - WINDOW - row) <= WINDOW
    bound = jnp.concatenate(
        [jnp.broadcast_to(sink[:, h : h + 1] * LOG2E, (WINDOW, 1)) for h in range(heads)], axis=0
    )
    ones = jnp.ones((3 * WINDOW, HEAD), bf16)
    pieces = [low[...]] + [lkv[pl.ds(i * WINDOW, WINDOW), :] for i in range(blocks)] + [high[...]]
    for i in range(blocks):
        keys = jnp.concatenate([p[:, :HEAD] for p in pieces[i : i + 3]], axis=0)
        values = jnp.concatenate([p[:, HEAD:] for p in pieces[i : i + 3]], axis=0)
        valid = band
        if i == 0 or i == blocks - 1:
            pos = offset + (i - 1) * WINDOW + col
            valid = band & (pos >= 0) & (pos < total_rows)
        rows = pl.ds(i * WINDOW, WINDOW)
        query = jnp.concatenate([lq[rows, h * HEAD : (h + 1) * HEAD] for h in range(heads)], axis=0)
        s = lax.dot_general(query, keys, ROWS_T, preferred_element_type=f32) * scale
        s = jnp.where(valid, s, MASKED)
        top = jnp.maximum(jnp.max(s, axis=-1, keepdims=True), bound)
        p = jnp.exp2(s - top).astype(bf16)
        o = dot(p, jnp.concatenate([values, ones], axis=1))
        o = (o[:, :HEAD] / (o[:, HEAD:] + jnp.exp2(bound - top))).astype(bf16)
        for h in range(heads):
            out[rows, h * HEAD : (h + 1) * HEAD] = o[h * WINDOW : (h + 1) * WINDOW]
    split_rows(out, keep, send)


def attend_body(tile, spans, first, last, *refs):
    q = refs[0]
    kvs = refs[1 : 1 + len(spans)]
    rest = refs[1 + len(spans) :]
    if not first:
        m_in, acc_in, rest = rest[0], rest[1], rest[2:]
    rows_all = q.shape[0]
    step = sum(spans) if last else max(spans)
    ones = jnp.ones((step, HEAD), bf16)
    groups = [list(zip(kvs, spans))] if last else [[pair] for pair in zip(kvs, spans)]
    for t in range(rows_all // tile):
        rows = pl.ds(t * tile, tile)
        query = q[rows, :]
        m = None if first else m_in[rows, :]
        acc = None if first else acc_in[rows, :]
        for group in groups:
            keys = jnp.concatenate([kv[pl.ds(0, span), :HEAD] for kv, span in group], axis=0)
            values = jnp.concatenate([kv[pl.ds(0, span), HEAD:] for kv, span in group], axis=0)
            s = lax.dot_general(query, keys, ROWS_T, preferred_element_type=f32)
            top = jnp.broadcast_to(jnp.max(s, axis=-1, keepdims=True), (tile, HEAD))
            new = top if m is None else jnp.maximum(m, top)
            p = jnp.exp2(s - jnp.concatenate([new] * (step // HEAD), axis=1)).astype(bf16)
            add = dot(p, jnp.concatenate([values, ones], axis=1))
            if m is None:
                acc = add
            else:
                factor = jnp.exp2(m - new)
                acc = acc * jnp.concatenate([factor, factor], axis=1) + add
            m = new
        if last:
            o = (acc[:, :HEAD] / acc[:, HEAD:]).astype(bf16)
            whole = rest[2]
            h, r = divmod(t * tile, whole.shape[0])
            whole[pl.ds(r, tile), h * HEAD : (h + 1) * HEAD] = o
        else:
            rest[0][rows, :] = m
            rest[1][rows, :] = acc
    if last:
        split_rows(rest[2], rest[0], rest[1])


def project_body(slots, keep, other, lkeep, lother, w, lw, w_other, lw_other, *outs):
    piece = outs[0].shape[-2]
    pieces = place()[2]
    weights = jnp.concatenate([w[...], w_other[...], lw[...], lw_other[...]], axis=0)
    for slot, out in zip(slots, outs):
        rows = pl.ds(pl.multiple_of(pieces[slot] * piece, 16), piece)
        part = jnp.concatenate([ref[rows, :] for ref in (keep, other, lkeep, lother)], axis=1)
        out[...] = dot(part, weights).astype(out.dtype)


def vmem(count):
    return [pl.BlockSpec(memory_space=pltpu.VMEM)] * count


def sds(shape, dtype):
    return jax.ShapeDtypeStruct(shape, dtype)


def cost(flops, transcendentals=0, bytes_accessed=0):
    return pl.CostEstimate(flops=int(flops), transcendentals=int(transcendentals), bytes_accessed=int(bytes_accessed))


def hbm(count):
    return [pl.BlockSpec(memory_space=pltpu.HBM)] * count


def in_hbm(*arrays):
    return [pltpu.with_memory_space_constraint(a, pltpu.HBM) for a in arrays]


def params(mib):
    return pltpu.CompilerParams(vmem_limit_bytes=mib * MIB)


def attend(q, blocks, state, last, row_count):
    rows, tile = q.shape[0], 256
    spans = tuple(b[1] for b in blocks)
    operands = [q] + [b[0] for b in blocks] + ([] if state is None else list(state))
    lanes = rows // row_count * HEAD
    if last:
        shape = (sds((row_count // 2, lanes), bf16),) * 2
    else:
        shape = (sds((rows, HEAD), f32), sds((rows, 2 * HEAD), f32))
    keys = sum(spans)
    return pl.pallas_call(
        functools.partial(attend_body, tile, spans, state is None, last),
        out_shape=shape,
        in_specs=vmem(len(operands)),
        out_specs=tuple(vmem(2)),
        scratch_shapes=[pltpu.VMEM((row_count, lanes), bf16)] if last else [],
        compiler_params=params(16),
        cost_estimate=cost(rows * keys * HEAD * 8, rows * keys),
        name="attend",
    )(*operands)


def project(slots, operands, piece, dtype):
    width = operands[-1].shape[1]
    depth = 4 * operands[0].shape[1]
    return pl.pallas_call(
        functools.partial(project_body, slots),
        out_shape=tuple(sds((piece, width), dtype) for _ in slots),
        in_specs=vmem(8),
        out_specs=tuple(vmem(len(slots))),
        compiler_params=params(8),
        cost_estimate=cost(2 * piece * width * depth * len(slots), 0, 4 * MIB),
        name="project",
    )(*operands)


def shards(
    tokens,
    norm_gain,
    grid_query_weight,
    grid_key_weight,
    grid_value_weight,
    grid_query_gain,
    grid_key_gain,
    local_query_weight,
    local_key_weight,
    local_value_weight,
    sink_logit,
    grid_out_weight,
    local_out_weight,
):
    row_count, width = tokens.shape
    n_sp = lax.axis_size("sp")
    n_tp = lax.axis_size("tp")
    total_rows = row_count * n_sp
    heads = grid_query_weight.shape[1] // HEAD
    row_np, col_np = turn_tables(total_rows, n_sp)
    row_tab, col_tab = jnp.asarray(row_np), jnp.asarray(col_np)

    tile = 128
    table_shape = (3, row_count // GRID_W, HEAD)
    normed, kv = pl.pallas_call(
        functools.partial(kv_body, tile),
        out_shape=(sds((row_count, width), bf16), sds((row_count, 2 * HEAD), bf16)),
        in_specs=hbm(7),
        out_specs=tuple(vmem(2)),
        scratch_shapes=[
            pltpu.VMEM((row_count, width), bf16),
            pltpu.VMEM((1, width), f32),
            pltpu.VMEM((width, HEAD), bf16),
            pltpu.VMEM((width, HEAD), bf16),
            pltpu.VMEM((1, HEAD), f32),
            pltpu.VMEM(table_shape, f32),
            pltpu.VMEM((3, GRID_W, HEAD), f32),
            pltpu.SemaphoreType.DMA((6 + row_count // tile,)),
        ],
        compiler_params=params(24),
        cost_estimate=cost(2 * row_count * width * 2 * HEAD, 0, 8 * MIB),
        name="keys",
    )(
        *in_hbm(
            tokens,
            norm_gain.reshape(1, width),
            grid_key_weight,
            grid_value_weight,
            grid_key_gain.reshape(1, HEAD),
            row_tab,
            col_tab,
        ),
    )

    forward = [(i, (i + 1) % n_sp) for i in range(n_sp)]
    backward = [(t, s) for s, t in forward]
    low = lax.ppermute(kv, "sp", forward)
    high = lax.ppermute(kv, "sp", backward)

    fold = HEAD ** (-0.5) * LOG2E
    q, lq, lkv, first_edge, last_edge = pl.pallas_call(
        functools.partial(q_body, 256),
        out_shape=(
            sds((heads * row_count, HEAD), bf16),
            sds((row_count, heads * HEAD), bf16),
            sds((row_count, 2 * HEAD), bf16),
            sds((WINDOW, 2 * HEAD), bf16),
            sds((WINDOW, 2 * HEAD), bf16),
        ),
        in_specs=vmem(1) + hbm(4) + vmem(1) + hbm(2),
        out_specs=tuple(vmem(5)),
        scratch_shapes=[
            pltpu.VMEM((width, heads * HEAD), bf16),
            pltpu.VMEM((width, heads * HEAD), bf16),
            pltpu.VMEM((width, HEAD), bf16),
            pltpu.VMEM((width, HEAD), bf16),
            pltpu.VMEM(table_shape, f32),
            pltpu.VMEM((3, GRID_W, HEAD), f32),
            pltpu.SemaphoreType.DMA((6,)),
        ],
        compiler_params=params(24),
        cost_estimate=cost(2 * row_count * width * 6 * HEAD, 0, 6 * MIB),
        name="queries",
    )(
        normed,
        *in_hbm(grid_query_weight, local_query_weight, local_key_weight, local_value_weight),
        (grid_query_gain * fold).reshape(1, HEAD),
        *in_hbm(row_tab, col_tab),
    )
    low_edge = lax.ppermute(last_edge, "sp", forward[:-1])
    high_edge = lax.ppermute(first_edge, "sp", backward[:-1])

    flip = [(i, i ^ 1) for i in range(n_tp)]
    first_hop = [(i, i ^ (2 + 2 * (i % 2))) for i in range(n_tp)]
    second_hop = [(i, i ^ (4 - 2 * (i % 2))) for i in range(n_tp)]
    w_other = lax.ppermute(grid_out_weight, "tp", flip)
    lw_other = lax.ppermute(local_out_weight, "tp", flip)

    state = attend(q, [(kv, row_count)], None, False, row_count)
    for _ in range(1, (n_sp - 1) // 2):
        next_low = lax.ppermute(low, "sp", forward)
        next_high = lax.ppermute(high, "sp", backward)
        state = attend(q, [(low, row_count), (high, row_count)], state, False, row_count)
        low, high = next_low, next_high
    half = row_count // 2
    cut_low, cut_high = low[:half], high[half:]
    far_low = lax.ppermute(cut_low, "sp", forward)
    far_high = lax.ppermute(cut_high, "sp", backward)

    lkeep, lsend = pl.pallas_call(
        functools.partial(local_body, row_count // WINDOW, total_rows),
        out_shape=(sds((row_count // 2, heads * HEAD), bf16),) * 2,
        in_specs=vmem(7),
        out_specs=tuple(vmem(2)),
        scratch_shapes=[pltpu.VMEM((row_count, heads * HEAD), bf16)],
        compiler_params=params(16),
        cost_estimate=cost(heads * row_count * 3 * WINDOW * HEAD * 8, heads * row_count * 3 * WINDOW),
        name="banded",
    )(sink_logit.reshape(1, heads), lq, lkv, low_edge, high_edge, cut_low, cut_high)
    lother = lax.ppermute(lsend, "tp", flip)
    state = attend(q, [(low, row_count), (high, row_count)], state, False, row_count)
    keep, send = attend(q, [(far_low, half), (far_high, half)], state, True, row_count)
    other = lax.ppermute(send, "tp", flip)

    piece = row_count // n_tp
    operands = (keep, other, lkeep, lother, grid_out_weight, local_out_weight, w_other, lw_other)
    (pass_on,) = project((0,), operands, piece, bf16)
    got_on = lax.ppermute(pass_on, "tp", first_hop)
    (direct,) = project((1,), operands, piece, bf16)
    got = lax.ppermute(direct, "tp", first_hop)
    next_part, own_part = project((2, 3), operands, piece, f32)
    got_next = lax.ppermute((next_part + got_on.astype(f32)).astype(bf16), "tp", second_hop)
    return (own_part + got.astype(f32) + got_next.astype(f32)).astype(bf16)


def solution(mesh):
    in_specs = (
        P("sp", None),
        P(),
        P(None, "tp"),
        P(None, "tp"),
        P(None, "tp"),
        P(),
        P(),
        P(None, "tp"),
        P(None, "tp"),
        P(None, "tp"),
        P("tp"),
        P("tp", None),
        P("tp", None),
    )
    out_specs = P(("sp", "tp"), None)
    return jax.shard_map(shards, mesh=mesh, in_specs=in_specs, out_specs=out_specs, check_vma=False)
```

```python
import functools
import math

import jax
import jax.numpy as jnp
import numpy as np
from jax import lax
from jax.experimental import pallas as pl
from jax.experimental.pallas import tpu as pltpu
from jax.sharding import PartitionSpec as P


HEAD = 128
WINDOW = 128
GRID_W = 64
EPSILON = 1e-06
ROPE_BASE = 10000.0
MASKED = -1e30
LOG2E = math.log2(math.e)
MIB = 1 << 20
COST = 0.3

bf16 = jnp.bfloat16
f32 = jnp.float32
ROWS_T = (((1,), (1,)), ((), ()))


def dot(a, b):
    return jnp.dot(a, b, preferred_element_type=f32)


def turn_tables(total_rows, seq_devices):
    half = HEAD // 2
    quarter = half // 2
    inverse = (ROPE_BASE ** (-np.arange(0, half, 2, dtype=np.float32) / np.float32(half))).astype(np.float32)

    def tables(count, first):
        angles = np.arange(count, dtype=np.float32)[:, None] * inverse
        out = np.zeros((3, count, HEAD), np.float32)
        base = 0 if first else half
        out[0, :, base : base + quarter] = np.cos(angles)
        out[0, :, base + quarter : base + half] = np.cos(angles)
        out[1, :, base : base + quarter] = -np.sin(angles)
        out[2, :, base + quarter : base + half] = np.sin(angles)
        return out

    rows = tables(total_rows // GRID_W, True)
    rows = rows.reshape(3, seq_devices, -1, HEAD).transpose(1, 0, 2, 3)
    return rows, tables(GRID_W, False)


def norm_turn(part, gain, row_tab, col_tab, first_row, grid_rows):
    x = part.astype(bf16).astype(f32)
    x = x * lax.rsqrt(jnp.mean(x * x, axis=-1, keepdims=True) + EPSILON) * gain

    def table(k):
        rows = row_tab[k, pl.ds(first_row, grid_rows), :]
        return (rows[:, None, :] + col_tab[k][None, :, :]).reshape(grid_rows * GRID_W, HEAD)

    quarter = HEAD // 4
    return (
        x * table(0)
        + pltpu.roll(x, HEAD - quarter, 1) * table(1)
        + pltpu.roll(x, quarter, 1) * table(2)
    )


def place():
    tp = lax.axis_index("tp")
    core, mine = tp % 2, tp // 2
    return lax.axis_index("sp"), core, (mine ^ 3, mine ^ (1 + core), mine ^ (2 - core), mine)


def start_copies(pairs, sems):
    copies = [pltpu.make_async_copy(src, dst, sems.at[i]) for i, (src, dst) in enumerate(pairs)]
    for copy in copies:
        copy.start()
    return copies


def norm_rows(x, gain):
    x = x.astype(f32)
    return (x * lax.rsqrt(jnp.mean(x * x, axis=-1, keepdims=True) + EPSILON) * gain).astype(bf16)


def kv_rows(first_row, normed, wk, wv, kgain, row_tab, col_tab, kv):
    y = dot(normed[...], jnp.concatenate([wk[...], wv[...]], axis=1))
    keys = norm_turn(y[:, :HEAD], kgain[...], row_tab, col_tab, first_row // GRID_W, normed.shape[0] // GRID_W)
    kv[...] = jnp.concatenate([keys, y[:, HEAD:]], axis=1).astype(bf16)


def first_keys_body(tile, tok, gain, kgain, row_tab, col_tab, wk, wv,
                    normed, kv, tok_b, gain_v, kgain_v, row_v, col_v, wk_v, wv_v, tok_v, sems):
    half = normed.shape[0]
    rows = [pl.ds(i, tile) for i in range(0, half, tile)]
    pairs = [(gain, gain_v)] + [(tok.at[r], tok_v.at[r]) for r in rows] + [(wk, wk_v), (wv, wv_v)]
    pairs += [(kgain, kgain_v), (row_tab.at[place()[0]], row_v), (col_tab, col_v)]
    copies = start_copies(pairs + [(tok.at[pl.ds(half, half)], tok_b)], sems)
    copies[0].wait()
    for r, copy in zip(rows, copies[1:]):
        copy.wait()
        normed[r, :] = norm_rows(tok_v[r, :], gain_v[...])
    for copy in copies[1 + len(rows) : -1]:
        copy.wait()
    kv_rows(0, normed, wk_v, wv_v, kgain_v, row_v, col_v, kv)
    copies[-1].wait()


def second_keys_body(tok, gain, kgain, row_tab, col_tab, wk, wv, wq, lwq, lwk, lwv, qgain,
                     normed, kv, wq_v, lwq_v, lwk_v, lwv_v, qgain_v, sems):
    pairs = [(wq, wq_v), (lwq, lwq_v), (lwk, lwk_v), (lwv, lwv_v), (qgain, qgain_v)]
    copies = start_copies(pairs, sems)
    normed[...] = norm_rows(tok[...], gain[...])
    kv_rows(normed.shape[0], normed, wk, wv, kgain, row_tab, col_tab, kv)
    for copy in copies:
        copy.wait()


def q_body(normed_a, normed_b, wq, lwq, lwk, lwv, qgain, row_tab, col_tab, q, lq, lkv, first_edge, last_edge):
    row_count = lq.shape[0]
    tile = row_count // 2
    heads = wq.shape[1] // HEAD
    gain = qgain[...] * (HEAD ** (-0.5) * LOG2E)
    for start, normed in ((0, normed_a), (tile, normed_b)):
        rows = pl.ds(start, tile)
        y = dot(normed[...], jnp.concatenate([wq[...], lwq[...], lwk[...], lwv[...]], axis=1))
        for h in range(heads):
            part = y[:, h * HEAD : (h + 1) * HEAD]
            turned = norm_turn(part, gain, row_tab, col_tab, start // GRID_W, tile // GRID_W)
            q[pl.ds(h * row_count + start, tile), :] = turned.astype(bf16)
        lq[rows, :] = y[:, heads * HEAD : 2 * heads * HEAD].astype(bf16)
        lkv[rows, :] = y[:, 2 * heads * HEAD :].astype(bf16)
    first_edge[...] = lkv[pl.ds(0, WINDOW), :]
    last_edge[...] = lkv[pl.ds(row_count - WINDOW, WINDOW), :]


def split_rows(whole, keep, send):
    piece = keep.shape[0] // (whole.shape[0] // keep.shape[0] * 2)
    count = keep.shape[0] // piece
    core = place()[1]
    for part, flip in ((keep, 0), (send, 1)):
        for i in range(count):
            start = pl.multiple_of(2 * i * piece + (core ^ flip) * piece, 16)
            part[pl.ds(i * piece, piece), :] = whole[pl.ds(start, piece), :]


def local_body(blocks, total_rows, sink, lq, lkv, low, high, keep, send, out):
    offset = place()[0] * (blocks * WINDOW)
    scale = HEAD ** (-0.5) * LOG2E
    heads = lq.shape[1] // HEAD
    shape = (heads * WINDOW, 3 * WINDOW)
    row = lax.broadcasted_iota(jnp.int32, shape, 0) % WINDOW
    col = lax.broadcasted_iota(jnp.int32, shape, 1)
    band = jnp.abs(col - WINDOW - row) <= WINDOW
    bound = jnp.concatenate(
        [jnp.broadcast_to(sink[:, h : h + 1] * LOG2E, (WINDOW, 1)) for h in range(heads)], axis=0
    )
    ones = jnp.ones((3 * WINDOW, HEAD), bf16)
    pieces = [low[...]] + [lkv[pl.ds(i * WINDOW, WINDOW), :] for i in range(blocks)] + [high[...]]
    for i in range(blocks):
        keys = jnp.concatenate([p[:, :HEAD] for p in pieces[i : i + 3]], axis=0)
        values = jnp.concatenate([p[:, HEAD:] for p in pieces[i : i + 3]], axis=0)
        valid = band
        if i == 0 or i == blocks - 1:
            pos = offset + (i - 1) * WINDOW + col
            valid = band & (pos >= 0) & (pos < total_rows)
        rows = pl.ds(i * WINDOW, WINDOW)
        query = jnp.concatenate([lq[rows, h * HEAD : (h + 1) * HEAD] for h in range(heads)], axis=0)
        s = lax.dot_general(query, keys, ROWS_T, preferred_element_type=f32) * scale
        s = jnp.where(valid, s, MASKED)
        top = jnp.maximum(jnp.max(s, axis=-1, keepdims=True), bound)
        p = jnp.exp2(s - top).astype(bf16)
        o = dot(p, jnp.concatenate([values, ones], axis=1))
        o = (o[:, :HEAD] / (o[:, HEAD:] + jnp.exp2(bound - top))).astype(bf16)
        for h in range(heads):
            out[rows, h * HEAD : (h + 1) * HEAD] = o[h * WINDOW : (h + 1) * WINDOW]
    split_rows(out, keep, send)


def softmax_step(query, pairs, m, acc):
    keys = jnp.concatenate([kv[:, :HEAD] for kv in pairs], axis=0)
    values = jnp.concatenate([kv[:, HEAD:] for kv in pairs], axis=0)
    values = jnp.concatenate([values, jnp.ones_like(values)], axis=1)
    s = lax.dot_general(query, keys, ROWS_T, preferred_element_type=f32)
    top = jnp.broadcast_to(jnp.max(s, axis=-1, keepdims=True), (query.shape[0], HEAD))
    new = top if m is None else jnp.maximum(m, top)
    p = jnp.exp2(s - jnp.concatenate([new] * (keys.shape[0] // HEAD), axis=1)).astype(bf16)
    add = dot(p, values)
    if m is not None:
        factor = jnp.exp2(m - new)
        add = acc * jnp.concatenate([factor, factor], axis=1) + add
    return new, add


def attend_body(tile, blocks, first, *refs):
    q = refs[0]
    kvs = refs[1 : 1 + 2 * blocks]
    rest = refs[1 + 2 * blocks :]
    if first:
        w, lw, m_out, acc_out, w_v, lw_v, sems = rest
        copies = start_copies([(w, w_v), (lw, lw_v)], sems)
    else:
        m_out, acc_out = rest[-2:]
    for start in range(0, q.shape[0], tile):
        rows = pl.ds(start, tile)
        m, acc = (None, None) if first else (rest[0][rows, :], rest[1][rows, :])
        for i in range(blocks):
            m, acc = softmax_step(q[rows, :], kvs[2 * i : 2 * i + 2], m, acc)
        m_out[rows, :] = m
        acc_out[rows, :] = acc
    if first:
        for copy in copies:
            copy.wait()


def finish_body(flips, row_count, q, kva, kvb, m_in, acc_in, keep, send):
    _, core, pieces = place()
    piece = keep.shape[0] // len(flips)
    for i, flip in enumerate(flips):
        out_rows = pl.ds(i * piece, piece)
        for h in range(q.shape[0] // row_count):
            start = h * row_count + (pieces[3] ^ flip) * 2 * piece
            rows = pl.ds(pl.multiple_of(start, 16), 2 * piece)
            _, acc = softmax_step(q[rows, :], (kva, kvb), m_in[rows, :], acc_in[rows, :])
            o = acc[:, :HEAD] / acc[:, HEAD:]
            lanes = slice(h * HEAD, (h + 1) * HEAD)
            keep[out_rows, lanes] = jnp.where(core == 0, o[:piece], o[piece:]).astype(bf16)
            send[out_rows, lanes] = jnp.where(core == 0, o[piece:], o[:piece]).astype(bf16)


def project_body(slots, keep, other, lkeep, lother, w, lw, w_other, lw_other, *outs):
    piece = outs[0].shape[-2]
    _, core, pieces = place()
    held = (0, 1 + core, 2 - core, 3)
    weights = jnp.concatenate([w[...], w_other[...], lw[...], lw_other[...]], axis=0)
    for slot, out in zip(slots, outs):
        rows = pl.ds(pl.multiple_of(held[slot] * piece, 16), piece)
        lrows = pl.ds(pl.multiple_of(pieces[slot] * piece, 16), piece)
        part = jnp.concatenate([keep[rows, :], other[rows, :], lkeep[lrows, :], lother[lrows, :]], axis=1)
        out[...] = dot(part, weights).astype(out.dtype)


def vmem(count):
    return [pl.BlockSpec(memory_space=pltpu.VMEM)] * count


def sds(shape, dtype):
    return jax.ShapeDtypeStruct(shape, dtype)


def cost(flops, transcendentals=0, bytes_accessed=0):
    return pl.CostEstimate(flops=int(COST * flops), transcendentals=int(transcendentals), bytes_accessed=int(bytes_accessed))


def hbm(count):
    return [pl.BlockSpec(memory_space=pltpu.HBM)] * count


def in_hbm(*arrays):
    return [pltpu.with_memory_space_constraint(a, pltpu.HBM) for a in arrays]


def params(mib):
    return pltpu.CompilerParams(vmem_limit_bytes=mib * MIB)


def attend(q, blocks, state, bring=()):
    rows = q.shape[0]
    operands = [q] + [part for block in blocks for part in block] + list(state or ())
    keys = sum(part.shape[0] for block in blocks for part in block)
    out_shape = (sds((rows, HEAD), f32), sds((rows, 2 * HEAD), f32)) + tuple(sds(a.shape, a.dtype) for a in bring)
    return pl.pallas_call(
        functools.partial(attend_body, 256, len(blocks), state is None),
        out_shape=out_shape,
        in_specs=vmem(len(operands)) + hbm(len(bring)),
        out_specs=tuple(vmem(len(out_shape))),
        scratch_shapes=[pltpu.SemaphoreType.DMA((len(bring),))] if bring else [],
        compiler_params=params(16),
        cost_estimate=cost(rows * keys * HEAD * 8, rows * keys),
    )(*operands, *in_hbm(*bring))


def finish(q, block, state, flips, row_count, piece):
    rows = q.shape[0]
    keys = 2 * block[0].shape[0]
    done = 2 * piece * len(flips) * rows // row_count
    return pl.pallas_call(
        functools.partial(finish_body, flips, row_count),
        out_shape=(sds((piece * len(flips), rows // row_count * HEAD), bf16),) * 2,
        in_specs=vmem(5),
        out_specs=tuple(vmem(2)),
        compiler_params=params(16),
        cost_estimate=cost(done * keys * HEAD * 8, done * keys),
        name="finish",
    )(q, *block, *state)


def project(slots, operands, piece, dtype):
    width = operands[-1].shape[1]
    depth = 4 * operands[0].shape[1]
    return pl.pallas_call(
        functools.partial(project_body, slots),
        out_shape=tuple(sds((piece, width), dtype) for _ in slots),
        in_specs=vmem(8),
        out_specs=tuple(vmem(len(slots))),
        compiler_params=params(8),
        cost_estimate=cost(2 * piece * width * depth * len(slots), 0, 4 * MIB),
        name="project",
    )(*operands)


def shards(
    tokens,
    norm_gain,
    grid_query_weight,
    grid_key_weight,
    grid_value_weight,
    grid_query_gain,
    grid_key_gain,
    local_query_weight,
    local_key_weight,
    local_value_weight,
    sink_logit,
    grid_out_weight,
    local_out_weight,
):
    row_count, width = tokens.shape
    n_sp = lax.axis_size("sp")
    n_tp = lax.axis_size("tp")
    total_rows = row_count * n_sp
    heads = grid_query_weight.shape[1] // HEAD
    row_np, col_np = turn_tables(total_rows, n_sp)
    row_tab, col_tab = jnp.asarray(row_np), jnp.asarray(col_np)

    tile = 128
    half = row_count // 2
    table_shape = (3, row_count // GRID_W, HEAD)

    tables = (sds((1, width), f32), sds((1, HEAD), f32), sds(table_shape, f32), sds((3, GRID_W, HEAD), f32))
    key_weights = grid_key_weight, grid_value_weight
    query_weights = grid_query_weight, local_query_weight, local_key_weight, local_value_weight
    rows_out = sds((half, width), bf16), sds((half, 2 * HEAD), bf16)
    key_cost = cost(2 * half * width * 2 * HEAD, 0, 4 * MIB)
    normed_a, kva, tokens_b, *shared = pl.pallas_call(
        functools.partial(first_keys_body, tile),
        out_shape=rows_out + (sds((half, width), bf16),) + tables + tuple(sds(w.shape, bf16) for w in key_weights),
        in_specs=hbm(7),
        out_specs=tuple(vmem(9)),
        scratch_shapes=[pltpu.VMEM((half, width), bf16), pltpu.SemaphoreType.DMA((7 + half // tile,))],
        compiler_params=params(16),
        cost_estimate=key_cost,
        name="keys_a",
    )(*in_hbm(tokens, norm_gain.reshape(1, width), grid_key_gain.reshape(1, HEAD), row_tab, col_tab, *key_weights))
    normed_b, kvb, *held = pl.pallas_call(
        second_keys_body,
        out_shape=rows_out + tuple(sds(w.shape, bf16) for w in query_weights) + (sds((1, HEAD), f32),),
        in_specs=vmem(7) + hbm(5),
        out_specs=tuple(vmem(7)),
        scratch_shapes=[pltpu.SemaphoreType.DMA((5,))],
        compiler_params=params(16),
        cost_estimate=key_cost,
        name="keys_b",
    )(tokens_b, *shared, *in_hbm(*query_weights, grid_query_gain.reshape(1, HEAD)))

    forward = [(i, (i + 1) % n_sp) for i in range(n_sp)]
    backward = [(t, s) for s, t in forward]


    def shift(low, high):
        low_a = lax.ppermute(low[0], "sp", forward)
        high_a = lax.ppermute(high[0], "sp", backward)
        low_b = lax.ppermute(low[1], "sp", forward)
        high_b = lax.ppermute(high[1], "sp", backward)
        return (low_a, low_b), (high_a, high_b)

    low, high = shift((kva, kvb), (kva, kvb))

    q, lq, lkv, first_edge, last_edge = pl.pallas_call(
        q_body,
        out_shape=(
            sds((heads * row_count, HEAD), bf16),
            sds((row_count, heads * HEAD), bf16),
            sds((row_count, 2 * HEAD), bf16),
            sds((WINDOW, 2 * HEAD), bf16),
            sds((WINDOW, 2 * HEAD), bf16),
        ),
        in_specs=vmem(9),
        out_specs=tuple(vmem(5)),
        compiler_params=params(16),
        cost_estimate=cost(2 * row_count * width * 6 * HEAD, 0, 6 * MIB),
        name="queries",
    )(normed_a, normed_b, *held, *shared[2:4])

    flip = [(i, i ^ 1) for i in range(n_tp)]
    first_hop = [(i, i ^ (2 + 2 * (i % 2))) for i in range(n_tp)]
    second_hop = [(i, i ^ (4 - 2 * (i % 2))) for i in range(n_tp)]
    low_edge = lax.ppermute(last_edge, "sp", forward[:-1])
    high_edge = lax.ppermute(first_edge, "sp", backward[:-1])
    *state, w_own, lw_own = attend(q, [(kva, kvb), (low[0], high[0])], None, (grid_out_weight, local_out_weight))
    w_other = lax.ppermute(w_own, "tp", flip)
    lw_other = lax.ppermute(lw_own, "tp", flip)
    for _ in range(1, (n_sp - 1) // 2):
        next_low, next_high = shift(low, high)
        state = attend(q, [(low[1], high[1]), (next_low[0], next_high[0])], state)
        low, high = next_low, next_high
    far = lax.ppermute(low[0], "sp", forward), lax.ppermute(high[1], "sp", backward)

    lkeep, lsend = pl.pallas_call(
        functools.partial(local_body, row_count // WINDOW, total_rows),
        out_shape=(sds((row_count // 2, heads * HEAD), bf16),) * 2,
        in_specs=vmem(5),
        out_specs=tuple(vmem(2)),
        scratch_shapes=[pltpu.VMEM((row_count, heads * HEAD), bf16)],
        compiler_params=params(16),
        cost_estimate=cost(heads * row_count * 3 * WINDOW * HEAD * 8, heads * row_count * 3 * WINDOW),
        name="banded",
    )(sink_logit.reshape(1, heads), lq, lkv, low_edge, high_edge)
    lother = lax.ppermute(lsend, "tp", flip)
    state = attend(q, [(low[1], high[1])], state)

    piece = row_count // n_tp
    keep, send = finish(q, far, state, (3, 1, 2, 0), row_count, piece)
    other = lax.ppermute(send, "tp", flip)
    operands = (keep, other, lkeep, lother, w_own, lw_own, w_other, lw_other)
    (pass_on,) = project((0,), operands, piece, bf16)
    got_on = lax.ppermute(pass_on, "tp", first_hop)
    (direct,) = project((1,), operands, piece, bf16)
    got = lax.ppermute(direct, "tp", first_hop)
    next_part, own_part = project((2, 3), operands, piece, f32)
    got_next = lax.ppermute((next_part + got_on.astype(f32)).astype(bf16), "tp", second_hop)
    return (own_part + got.astype(f32) + got_next.astype(f32)).astype(bf16)


def solution(mesh):
    in_specs = (
        P("sp", None),
        P(),
        P(None, "tp"),
        P(None, "tp"),
        P(None, "tp"),
        P(),
        P(),
        P(None, "tp"),
        P(None, "tp"),
        P(None, "tp"),
        P("tp"),
        P("tp", None),
        P("tp", None),
    )
    out_specs = P(("sp", "tp"), None)

    return jax.shard_map(shards, mesh=mesh, in_specs=in_specs, out_specs=out_specs, check_vma=False)
```

```python
import functools
import math

import jax
import jax.numpy as jnp
import numpy as np
from jax import lax
from jax.experimental import pallas as pl
from jax.experimental.pallas import tpu as pltpu
from jax.sharding import PartitionSpec as P


HEAD = 128
WINDOW = 128
GRID_W = 64
EPSILON = 1e-06
ROPE_BASE = 10000.0
MASKED = -1e30
LOG2E = math.log2(math.e)
MIB = 1 << 20
COST = 0.3

bf16 = jnp.bfloat16
f32 = jnp.float32
ROWS_T = (((1,), (1,)), ((), ()))


def dot(a, b):
    return jnp.dot(a, b, preferred_element_type=f32)


def turn_tables(total_rows, seq_devices):
    half = HEAD // 2
    quarter = half // 2
    inverse = (ROPE_BASE ** (-np.arange(0, half, 2, dtype=np.float32) / np.float32(half))).astype(np.float32)

    def tables(count, first):
        angles = np.arange(count, dtype=np.float32)[:, None] * inverse
        out = np.zeros((3, count, HEAD), np.float32)
        base = 0 if first else half
        out[0, :, base : base + quarter] = np.cos(angles)
        out[0, :, base + quarter : base + half] = np.cos(angles)
        out[1, :, base : base + quarter] = -np.sin(angles)
        out[2, :, base + quarter : base + half] = np.sin(angles)
        return out

    rows = tables(total_rows // GRID_W, True)
    rows = rows.reshape(3, seq_devices, -1, HEAD).transpose(1, 0, 2, 3)
    return rows, tables(GRID_W, False)


def norm_turn(part, gain, row_tab, col_tab, first_row, grid_rows):
    x = part.astype(bf16).astype(f32)
    x = x * lax.rsqrt(jnp.mean(x * x, axis=-1, keepdims=True) + EPSILON) * gain

    def table(k):
        rows = row_tab[k, pl.ds(first_row, grid_rows), :]
        return (rows[:, None, :] + col_tab[k][None, :, :]).reshape(grid_rows * GRID_W, HEAD)

    quarter = HEAD // 4
    return (
        x * table(0)
        + pltpu.roll(x, HEAD - quarter, 1) * table(1)
        + pltpu.roll(x, quarter, 1) * table(2)
    )


def place():
    tp = lax.axis_index("tp")
    core, mine = tp % 2, tp // 2
    return lax.axis_index("sp"), core, (mine ^ 3, mine ^ (1 + core), mine ^ (2 - core), mine)


def start_copies(pairs, sems):
    copies = [pltpu.make_async_copy(src, dst, sems.at[i]) for i, (src, dst) in enumerate(pairs)]
    for copy in copies:
        copy.start()
    return copies


def norm_rows(x, gain):
    x = x.astype(f32)
    return (x * lax.rsqrt(jnp.mean(x * x, axis=-1, keepdims=True) + EPSILON) * gain).astype(bf16)


def kv_rows(first_row, normed, wk, wv, kgain, row_tab, col_tab, kv):
    y = dot(normed[...], jnp.concatenate([wk[...], wv[...]], axis=1))
    keys = norm_turn(y[:, :HEAD], kgain[...], row_tab, col_tab, first_row // GRID_W, normed.shape[0] // GRID_W)
    kv[...] = jnp.concatenate([keys, y[:, HEAD:]], axis=1).astype(bf16)


def first_keys_body(tile, tok, gain, kgain, row_tab, col_tab, wk, wv,
                    normed, kv, tok_b, gain_v, kgain_v, row_v, col_v, wk_v, wv_v, tok_v, sems):
    half = normed.shape[0]
    rows = [pl.ds(i, tile) for i in range(0, half, tile)]
    pairs = [(gain, gain_v)] + [(tok.at[r], tok_v.at[r]) for r in rows] + [(wk, wk_v), (wv, wv_v)]
    pairs += [(kgain, kgain_v), (row_tab.at[place()[0]], row_v), (col_tab, col_v)]
    copies = start_copies(pairs + [(tok.at[pl.ds(half, half)], tok_b)], sems)
    copies[0].wait()
    for r, copy in zip(rows, copies[1:]):
        copy.wait()
        normed[r, :] = norm_rows(tok_v[r, :], gain_v[...])
    for copy in copies[1 + len(rows) : -1]:
        copy.wait()
    kv_rows(0, normed, wk_v, wv_v, kgain_v, row_v, col_v, kv)
    copies[-1].wait()


def second_keys_body(tok, gain, kgain, row_tab, col_tab, wk, wv, wq, lwq, lwk, lwv, qgain,
                     normed, kv, wq_v, lwq_v, lwk_v, lwv_v, qgain_v, sems):
    pairs = [(wq, wq_v), (lwq, lwq_v), (lwk, lwk_v), (lwv, lwv_v), (qgain, qgain_v)]
    copies = start_copies(pairs, sems)
    normed[...] = norm_rows(tok[...], gain[...])
    kv_rows(normed.shape[0], normed, wk, wv, kgain, row_tab, col_tab, kv)
    for copy in copies:
        copy.wait()


def q_body(normed_a, normed_b, wq, lwq, lwk, lwv, qgain, row_tab, col_tab, q, lq, lkv, first_edge, last_edge):
    row_count = lq.shape[0]
    tile = row_count // 2
    heads = wq.shape[1] // HEAD
    gain = qgain[...] * (HEAD ** (-0.5) * LOG2E)
    for start, normed in ((0, normed_a), (tile, normed_b)):
        rows = pl.ds(start, tile)
        y = dot(normed[...], jnp.concatenate([wq[...], lwq[...], lwk[...], lwv[...]], axis=1))
        for h in range(heads):
            part = y[:, h * HEAD : (h + 1) * HEAD]
            turned = norm_turn(part, gain, row_tab, col_tab, start // GRID_W, tile // GRID_W)
            q[pl.ds(h * row_count + start, tile), :] = turned.astype(bf16)
        lq[rows, :] = y[:, heads * HEAD : 2 * heads * HEAD].astype(bf16)
        lkv[rows, :] = y[:, 2 * heads * HEAD :].astype(bf16)
    first_edge[...] = lkv[pl.ds(0, WINDOW), :]
    last_edge[...] = lkv[pl.ds(row_count - WINDOW, WINDOW), :]


def split_rows(whole, keep, send):
    piece = keep.shape[0] // (whole.shape[0] // keep.shape[0] * 2)
    count = keep.shape[0] // piece
    core = place()[1]
    for part, flip in ((keep, 0), (send, 1)):
        for i in range(count):
            start = pl.multiple_of(2 * i * piece + (core ^ flip) * piece, 16)
            part[pl.ds(i * piece, piece), :] = whole[pl.ds(start, piece), :]


def local_body(blocks, total_rows, sink, lq, lkv, low, high, keep, send, out):
    offset = place()[0] * (blocks * WINDOW)
    scale = HEAD ** (-0.5) * LOG2E
    heads = lq.shape[1] // HEAD
    shape = (heads * WINDOW, 3 * WINDOW)
    row = lax.broadcasted_iota(jnp.int32, shape, 0) % WINDOW
    col = lax.broadcasted_iota(jnp.int32, shape, 1)
    band = jnp.abs(col - WINDOW - row) <= WINDOW
    bound = jnp.concatenate(
        [jnp.broadcast_to(sink[:, h : h + 1] * LOG2E, (WINDOW, 1)) for h in range(heads)], axis=0
    )
    ones = jnp.ones((3 * WINDOW, HEAD), bf16)
    pieces = [low[...]] + [lkv[pl.ds(i * WINDOW, WINDOW), :] for i in range(blocks)] + [high[...]]
    for i in range(blocks):
        keys = jnp.concatenate([p[:, :HEAD] for p in pieces[i : i + 3]], axis=0)
        values = jnp.concatenate([p[:, HEAD:] for p in pieces[i : i + 3]], axis=0)
        valid = band
        if i == 0 or i == blocks - 1:
            pos = offset + (i - 1) * WINDOW + col
            valid = band & (pos >= 0) & (pos < total_rows)
        rows = pl.ds(i * WINDOW, WINDOW)
        query = jnp.concatenate([lq[rows, h * HEAD : (h + 1) * HEAD] for h in range(heads)], axis=0)
        s = lax.dot_general(query, keys, ROWS_T, preferred_element_type=f32) * scale
        s = jnp.where(valid, s, MASKED)
        top = jnp.maximum(jnp.max(s, axis=-1, keepdims=True), bound)
        p = jnp.exp2(s - top).astype(bf16)
        o = dot(p, jnp.concatenate([values, ones], axis=1))
        o = (o[:, :HEAD] / (o[:, HEAD:] + jnp.exp2(bound - top))).astype(bf16)
        for h in range(heads):
            out[rows, h * HEAD : (h + 1) * HEAD] = o[h * WINDOW : (h + 1) * WINDOW]
    split_rows(out, keep, send)


def softmax_step(query, pairs, m, acc):
    keys = jnp.concatenate([kv[:, :HEAD] for kv in pairs], axis=0)
    values = jnp.concatenate([kv[:, HEAD:] for kv in pairs], axis=0)
    values = jnp.concatenate([values, jnp.ones_like(values)], axis=1)
    s = lax.dot_general(query, keys, ROWS_T, preferred_element_type=f32)
    top = jnp.broadcast_to(jnp.max(s, axis=-1, keepdims=True), (query.shape[0], HEAD))
    new = top if m is None else jnp.maximum(m, top)
    p = jnp.exp2(s - jnp.concatenate([new] * (keys.shape[0] // HEAD), axis=1)).astype(bf16)
    add = dot(p, values)
    if m is not None:
        factor = jnp.exp2(m - new)
        add = acc * jnp.concatenate([factor, factor], axis=1) + add
    return new, add


def attend_body(tile, parts, first, *refs):
    q = refs[0]
    kvs = refs[1 : 1 + sum(parts)]
    rest = refs[1 + sum(parts) :]
    if first:
        w, lw, m_out, acc_out, w_v, lw_v, sems = rest
        copies = start_copies([(w, w_v), (lw, lw_v)], sems)
    else:
        m_out, acc_out = rest[-2:]
    for start in range(0, q.shape[0], tile):
        rows = pl.ds(start, tile)
        m, acc = (None, None) if first else (rest[0][rows, :], rest[1][rows, :])
        used = 0
        for count in parts:
            m, acc = softmax_step(q[rows, :], kvs[used : used + count], m, acc)
            used += count
        m_out[rows, :] = m
        acc_out[rows, :] = acc
    if first:
        for copy in copies:
            copy.wait()


def finish_body(flips, row_count, q, kv, m_in, acc_in, keep, send):
    _, core, pieces = place()
    piece = keep.shape[0] // len(flips)
    for i, flip in enumerate(flips):
        out_rows = pl.ds(i * piece, piece)
        for h in range(q.shape[0] // row_count):
            start = h * row_count + (pieces[3] ^ flip) * 2 * piece
            rows = pl.ds(pl.multiple_of(start, 16), 2 * piece)
            _, acc = softmax_step(q[rows, :], (kv,), m_in[rows, :], acc_in[rows, :])
            o = acc[:, :HEAD] / acc[:, HEAD:]
            lanes = slice(h * HEAD, (h + 1) * HEAD)
            keep[out_rows, lanes] = jnp.where(core == 0, o[:piece], o[piece:]).astype(bf16)
            send[out_rows, lanes] = jnp.where(core == 0, o[piece:], o[:piece]).astype(bf16)


def project_body(slots, keep, other, lkeep, lother, w, lw, w_other, lw_other, *outs):
    piece = outs[0].shape[-2]
    _, core, pieces = place()
    held = (0, core, 1 - core, 2)
    weights = jnp.concatenate([w[...], w_other[...], lw[...], lw_other[...]], axis=0)
    for slot, out in zip(slots, outs):
        rows = pl.ds(pl.multiple_of(held[slot] * piece, 16), piece)
        lrows = pl.ds(pl.multiple_of(pieces[slot] * piece, 16), piece)
        part = jnp.concatenate([keep[rows, :], other[rows, :], lkeep[lrows, :], lother[lrows, :]], axis=1)
        out[...] = dot(part, weights).astype(out.dtype)


def vmem(count):
    return [pl.BlockSpec(memory_space=pltpu.VMEM)] * count


def sds(shape, dtype):
    return jax.ShapeDtypeStruct(shape, dtype)


def cost(flops, transcendentals=0, bytes_accessed=0):
    return pl.CostEstimate(flops=int(COST * flops), transcendentals=int(transcendentals), bytes_accessed=int(bytes_accessed))


def hbm(count):
    return [pl.BlockSpec(memory_space=pltpu.HBM)] * count


def in_hbm(*arrays):
    return [pltpu.with_memory_space_constraint(a, pltpu.HBM) for a in arrays]


def params(mib):
    return pltpu.CompilerParams(vmem_limit_bytes=mib * MIB)


def attend(q, blocks, state, bring=()):
    rows = q.shape[0]
    operands = [q] + [part for block in blocks for part in block] + list(state or ())
    keys = sum(part.shape[0] for block in blocks for part in block)
    out_shape = (sds((rows, HEAD), f32), sds((rows, 2 * HEAD), f32)) + tuple(sds(a.shape, a.dtype) for a in bring)
    return pl.pallas_call(
        functools.partial(attend_body, 256, tuple(len(block) for block in blocks), state is None),
        out_shape=out_shape,
        in_specs=vmem(len(operands)) + hbm(len(bring)),
        out_specs=tuple(vmem(len(out_shape))),
        scratch_shapes=[pltpu.SemaphoreType.DMA((len(bring),))] if bring else [],
        compiler_params=params(16),
        cost_estimate=cost(rows * keys * HEAD * 8, rows * keys),
    )(*operands, *in_hbm(*bring))


def finish(q, kv, state, flips, row_count, piece):
    rows = q.shape[0]
    keys = kv.shape[0]
    done = 2 * piece * len(flips) * rows // row_count
    return pl.pallas_call(
        functools.partial(finish_body, flips, row_count),
        out_shape=(sds((piece * len(flips), rows // row_count * HEAD), bf16),) * 2,
        in_specs=vmem(4),
        out_specs=tuple(vmem(2)),
        compiler_params=params(16),
        cost_estimate=cost(done * keys * HEAD * 8, done * keys),
    )(q, kv, *state)


def project(slots, operands, piece, dtype):
    width = operands[-1].shape[1]
    depth = 4 * operands[0].shape[1]
    return pl.pallas_call(
        functools.partial(project_body, slots),
        out_shape=tuple(sds((piece, width), dtype) for _ in slots),
        in_specs=vmem(8),
        out_specs=tuple(vmem(len(slots))),
        compiler_params=params(8),
        cost_estimate=cost(2 * piece * width * depth * len(slots), 0, 4 * MIB),
    )(*operands)


def shards(
    tokens,
    norm_gain,
    grid_query_weight,
    grid_key_weight,
    grid_value_weight,
    grid_query_gain,
    grid_key_gain,
    local_query_weight,
    local_key_weight,
    local_value_weight,
    sink_logit,
    grid_out_weight,
    local_out_weight,
):
    row_count, width = tokens.shape
    n_sp = lax.axis_size("sp")
    n_tp = lax.axis_size("tp")
    total_rows = row_count * n_sp
    heads = grid_query_weight.shape[1] // HEAD
    row_np, col_np = turn_tables(total_rows, n_sp)
    row_tab, col_tab = jnp.asarray(row_np), jnp.asarray(col_np)

    tile = 128
    half = row_count // 2
    table_shape = (3, row_count // GRID_W, HEAD)

    tables = (sds((1, width), f32), sds((1, HEAD), f32), sds(table_shape, f32), sds((3, GRID_W, HEAD), f32))
    key_weights = grid_key_weight, grid_value_weight
    query_weights = grid_query_weight, local_query_weight, local_key_weight, local_value_weight
    rows_out = sds((half, width), bf16), sds((half, 2 * HEAD), bf16)
    key_cost = cost(2 * half * width * 2 * HEAD, 0, 4 * MIB)
    normed_a, kva, tokens_b, *shared = pl.pallas_call(
        functools.partial(first_keys_body, tile),
        out_shape=rows_out + (sds((half, width), bf16),) + tables + tuple(sds(w.shape, bf16) for w in key_weights),
        in_specs=hbm(7),
        out_specs=tuple(vmem(9)),
        scratch_shapes=[pltpu.VMEM((half, width), bf16), pltpu.SemaphoreType.DMA((7 + half // tile,))],
        compiler_params=params(16),
        cost_estimate=key_cost,
        name="keys_a",
    )(*in_hbm(tokens, norm_gain.reshape(1, width), grid_key_gain.reshape(1, HEAD), row_tab, col_tab, *key_weights))
    normed_b, kvb, *held = pl.pallas_call(
        second_keys_body,
        out_shape=rows_out + tuple(sds(w.shape, bf16) for w in query_weights) + (sds((1, HEAD), f32),),
        in_specs=vmem(7) + hbm(5),
        out_specs=tuple(vmem(7)),
        scratch_shapes=[pltpu.SemaphoreType.DMA((5,))],
        compiler_params=params(16),
        cost_estimate=key_cost,
        name="keys_b",
    )(tokens_b, *shared, *in_hbm(*query_weights, grid_query_gain.reshape(1, HEAD)))

    forward = [(i, (i + 1) % n_sp) for i in range(n_sp)]
    backward = [(t, s) for s, t in forward]


    def shift(low, high):
        low_a = lax.ppermute(low[0], "sp", forward)
        high_b = lax.ppermute(high[1], "sp", backward)
        low_b = lax.ppermute(low[1], "sp", forward)
        high_a = lax.ppermute(high[0], "sp", backward)
        return (low_a, low_b), (high_a, high_b)

    low, high = shift((kva, kvb), (kva, kvb))

    q, lq, lkv, first_edge, last_edge = pl.pallas_call(
        q_body,
        out_shape=(
            sds((heads * row_count, HEAD), bf16),
            sds((row_count, heads * HEAD), bf16),
            sds((row_count, 2 * HEAD), bf16),
            sds((WINDOW, 2 * HEAD), bf16),
            sds((WINDOW, 2 * HEAD), bf16),
        ),
        in_specs=vmem(9),
        out_specs=tuple(vmem(5)),
        compiler_params=params(16),
        cost_estimate=cost(2 * row_count * width * 6 * HEAD, 0, 6 * MIB),
        name="queries",
    )(normed_a, normed_b, *held, *shared[2:4])

    flip = [(i, i ^ 1) for i in range(n_tp)]
    first_hop = [(i, i ^ (2 + 2 * (i % 2))) for i in range(n_tp)]
    second_hop = [(i, i ^ (4 - 2 * (i % 2))) for i in range(n_tp)]
    low_edge = lax.ppermute(last_edge, "sp", forward[:-1])
    high_edge = lax.ppermute(first_edge, "sp", backward[:-1])
    *state, w_own, lw_own = attend(q, [(kva, kvb), (low[0], high[1])], None, (grid_out_weight, local_out_weight))
    w_other = lax.ppermute(w_own, "tp", flip)
    lw_other = lax.ppermute(lw_own, "tp", flip)
    for _ in range(1, (n_sp - 1) // 2):
        next_low, next_high = shift(low, high)
        state = attend(q, [(low[1], high[0]), (next_low[0], next_high[1])], state)
        low, high = next_low, next_high
    far = lax.ppermute(low[0], "sp", forward), lax.ppermute(high[1], "sp", backward)

    lkeep, lsend = pl.pallas_call(
        functools.partial(local_body, row_count // WINDOW, total_rows),
        out_shape=(sds((row_count // 2, heads * HEAD), bf16),) * 2,
        in_specs=vmem(5),
        out_specs=tuple(vmem(2)),
        scratch_shapes=[pltpu.VMEM((row_count, heads * HEAD), bf16)],
        compiler_params=params(16),
        cost_estimate=cost(heads * row_count * 3 * WINDOW * HEAD * 8, heads * row_count * 3 * WINDOW),
        name="banded",
    )(sink_logit.reshape(1, heads), lq, lkv, low_edge, high_edge)
    lother = lax.ppermute(lsend, "tp", flip)
    state = attend(q, [(low[1], high[0])], state)

    piece = row_count // n_tp
    state = attend(q, [(far[0],)], state)
    keep, send = finish(q, far[1], state, (3,), row_count, piece)
    other = lax.ppermute(send, "tp", flip)
    keep_rest, send_rest = finish(q, far[1], state, (1, 2, 0), row_count, piece)
    other_rest = lax.ppermute(send_rest, "tp", flip)

    fixed = (lkeep, lother, w_own, lw_own, w_other, lw_other)
    (pass_on,) = project((0,), (keep, other) + fixed, piece, bf16)
    got_on = lax.ppermute(pass_on, "tp", first_hop)
    next_part, own_part = project((2, 3), (keep_rest, other_rest) + fixed, piece, f32)
    (direct,) = project((1,), (keep_rest, other_rest) + fixed, piece, bf16)
    got = lax.ppermute(direct, "tp", first_hop)
    got_next = lax.ppermute((next_part + got_on.astype(f32)).astype(bf16), "tp", second_hop)
    summed = lax.optimization_barrier(own_part + got.astype(f32))
    return (summed + got_next.astype(f32)).astype(bf16)


def solution(mesh):
    in_specs = (
        P("sp", None),
        P(),
        P(None, "tp"),
        P(None, "tp"),
        P(None, "tp"),
        P(),
        P(),
        P(None, "tp"),
        P(None, "tp"),
        P(None, "tp"),
        P("tp"),
        P("tp", None),
        P("tp", None),
    )
    out_specs = P(("sp", "tp"), None)

    return jax.shard_map(shards, mesh=mesh, in_specs=in_specs, out_specs=out_specs, check_vma=False)
```

```python
import functools
import math

import jax
import jax.numpy as jnp
import numpy as np
from jax import lax
from jax.experimental import pallas as pl
from jax.experimental.pallas import tpu as pltpu
from jax.sharding import PartitionSpec as P


HEAD = 128
WINDOW = 128
GRID_W = 64
EPSILON = 1e-06
ROPE_BASE = 10000.0
MASKED = -1e30
LOG2E = math.log2(math.e)
MIB = 1 << 20
COST = 0.3

bf16 = jnp.bfloat16
f32 = jnp.float32
ROWS_T = (((1,), (1,)), ((), ()))


def dot(a, b):
    return jnp.dot(a, b, preferred_element_type=f32)


def turn_tables(total_rows, seq_devices):
    half = HEAD // 2
    quarter = half // 2
    inverse = (ROPE_BASE ** (-np.arange(0, half, 2, dtype=np.float32) / np.float32(half))).astype(np.float32)

    def tables(count, first):
        angles = np.arange(count, dtype=np.float32)[:, None] * inverse
        out = np.zeros((3, count, HEAD), np.float32)
        base = 0 if first else half
        out[0, :, base : base + quarter] = np.cos(angles)
        out[0, :, base + quarter : base + half] = np.cos(angles)
        out[1, :, base : base + quarter] = -np.sin(angles)
        out[2, :, base + quarter : base + half] = np.sin(angles)
        return out

    rows = tables(total_rows // GRID_W, True)
    rows = rows.reshape(3, seq_devices, -1, HEAD).transpose(1, 0, 2, 3)
    return rows, tables(GRID_W, False)


def norm_turn(part, gain, row_tab, col_tab, first_row, grid_rows):
    x = part.astype(bf16).astype(f32)
    x = x * lax.rsqrt(jnp.mean(x * x, axis=-1, keepdims=True) + EPSILON) * gain

    def table(k):
        rows = row_tab[k, pl.ds(first_row, grid_rows), :]
        return (rows[:, None, :] + col_tab[k][None, :, :]).reshape(grid_rows * GRID_W, HEAD)

    quarter = HEAD // 4
    return (
        x * table(0)
        + pltpu.roll(x, HEAD - quarter, 1) * table(1)
        + pltpu.roll(x, quarter, 1) * table(2)
    )


def place():
    tp = lax.axis_index("tp")
    core, mine = tp % 2, tp // 2
    return lax.axis_index("sp"), core, (mine ^ 3, mine ^ (1 + core), mine ^ (2 - core), mine)


def start_copies(pairs, sems):
    copies = [pltpu.make_async_copy(src, dst, sems.at[i]) for i, (src, dst) in enumerate(pairs)]
    for copy in copies:
        copy.start()
    return copies


def norm_rows(x, gain):
    x = x.astype(f32)
    return (x * lax.rsqrt(jnp.mean(x * x, axis=-1, keepdims=True) + EPSILON) * gain).astype(bf16)


def kv_rows(first_row, normed, wk, wv, kgain, row_tab, col_tab, kv):
    y = dot(normed[...], jnp.concatenate([wk[...], wv[...]], axis=1))
    keys = norm_turn(y[:, :HEAD], kgain[...], row_tab, col_tab, first_row // GRID_W, normed.shape[0] // GRID_W)
    kv[...] = jnp.concatenate([keys, y[:, HEAD:]], axis=1).astype(bf16)


def first_keys_body(tile, tok, gain, kgain, row_tab, col_tab, wk, wv,
                    normed, kv, tok_b, gain_v, kgain_v, row_v, col_v, wk_v, wv_v, tok_v, sems):
    half = normed.shape[0]
    rows = [pl.ds(i, tile) for i in range(0, half, tile)]
    pairs = [(gain, gain_v)] + [(tok.at[r], tok_v.at[r]) for r in rows] + [(wk, wk_v), (wv, wv_v)]
    pairs += [(kgain, kgain_v), (row_tab.at[place()[0]], row_v), (col_tab, col_v)]
    copies = start_copies(pairs + [(tok.at[pl.ds(half, half)], tok_b)], sems)
    copies[0].wait()
    for r, copy in zip(rows, copies[1:]):
        copy.wait()
        normed[r, :] = norm_rows(tok_v[r, :], gain_v[...])
    for copy in copies[1 + len(rows) : -1]:
        copy.wait()
    kv_rows(0, normed, wk_v, wv_v, kgain_v, row_v, col_v, kv)
    copies[-1].wait()


def second_keys_body(tok, gain, kgain, row_tab, col_tab, wk, wv, wq, lwq, lwk, lwv, qgain,
                     normed, kv, wq_v, lwq_v, lwk_v, lwv_v, qgain_v, sems):
    pairs = [(wq, wq_v), (lwq, lwq_v), (lwk, lwk_v), (lwv, lwv_v), (qgain, qgain_v)]
    copies = start_copies(pairs, sems)
    normed[...] = norm_rows(tok[...], gain[...])
    kv_rows(normed.shape[0], normed, wk, wv, kgain, row_tab, col_tab, kv)
    for copy in copies:
        copy.wait()


def q_body(normed_a, normed_b, wq, lwq, lwk, lwv, qgain, row_tab, col_tab, q, lq, lkv, first_edge, last_edge):
    row_count = lq.shape[0]
    tile = row_count // 2
    heads = wq.shape[1] // HEAD
    gain = qgain[...] * (HEAD ** (-0.5) * LOG2E)
    for start, normed in ((0, normed_a), (tile, normed_b)):
        rows = pl.ds(start, tile)
        y = dot(normed[...], jnp.concatenate([wq[...], lwq[...], lwk[...], lwv[...]], axis=1))
        for h in range(heads):
            part = y[:, h * HEAD : (h + 1) * HEAD]
            turned = norm_turn(part, gain, row_tab, col_tab, start // GRID_W, tile // GRID_W)
            q[pl.ds(h * row_count + start, tile), :] = turned.astype(bf16)
        lq[rows, :] = y[:, heads * HEAD : 2 * heads * HEAD].astype(bf16)
        lkv[rows, :] = y[:, 2 * heads * HEAD :].astype(bf16)
    first_edge[...] = lkv[pl.ds(0, WINDOW), :]
    last_edge[...] = lkv[pl.ds(row_count - WINDOW, WINDOW), :]


def split_rows(whole, keep, send):
    piece = keep.shape[0] // (whole.shape[0] // keep.shape[0] * 2)
    count = keep.shape[0] // piece
    core = place()[1]
    for part, flip in ((keep, 0), (send, 1)):
        for i in range(count):
            start = pl.multiple_of(2 * i * piece + (core ^ flip) * piece, 16)
            part[pl.ds(i * piece, piece), :] = whole[pl.ds(start, piece), :]


def local_body(blocks, total_rows, sink, lq, lkv, low, high, keep, send, out):
    offset = place()[0] * (blocks * WINDOW)
    scale = HEAD ** (-0.5) * LOG2E
    heads = lq.shape[1] // HEAD
    shape = (heads * WINDOW, 3 * WINDOW)
    row = lax.broadcasted_iota(jnp.int32, shape, 0) % WINDOW
    col = lax.broadcasted_iota(jnp.int32, shape, 1)
    band = jnp.abs(col - WINDOW - row) <= WINDOW
    bound = jnp.concatenate(
        [jnp.broadcast_to(sink[:, h : h + 1] * LOG2E, (WINDOW, 1)) for h in range(heads)], axis=0
    )
    ones = jnp.ones((3 * WINDOW, HEAD), bf16)
    pieces = [low[...]] + [lkv[pl.ds(i * WINDOW, WINDOW), :] for i in range(blocks)] + [high[...]]
    for i in range(blocks):
        keys = jnp.concatenate([p[:, :HEAD] for p in pieces[i : i + 3]], axis=0)
        values = jnp.concatenate([p[:, HEAD:] for p in pieces[i : i + 3]], axis=0)
        valid = band
        if i == 0 or i == blocks - 1:
            pos = offset + (i - 1) * WINDOW + col
            valid = band & (pos >= 0) & (pos < total_rows)
        rows = pl.ds(i * WINDOW, WINDOW)
        query = jnp.concatenate([lq[rows, h * HEAD : (h + 1) * HEAD] for h in range(heads)], axis=0)
        s = lax.dot_general(query, keys, ROWS_T, preferred_element_type=f32) * scale
        s = jnp.where(valid, s, MASKED)
        top = jnp.maximum(jnp.max(s, axis=-1, keepdims=True), bound)
        p = jnp.exp2(s - top).astype(bf16)
        o = dot(p, jnp.concatenate([values, ones], axis=1))
        o = (o[:, :HEAD] / (o[:, HEAD:] + jnp.exp2(bound - top))).astype(bf16)
        for h in range(heads):
            out[rows, h * HEAD : (h + 1) * HEAD] = o[h * WINDOW : (h + 1) * WINDOW]
    split_rows(out, keep, send)


def softmax_step(query, pairs, m, acc):
    keys = jnp.concatenate([kv[:, :HEAD] for kv in pairs], axis=0)
    values = jnp.concatenate([kv[:, HEAD:] for kv in pairs], axis=0)
    values = jnp.concatenate([values, jnp.ones_like(values)], axis=1)
    s = lax.dot_general(query, keys, ROWS_T, preferred_element_type=f32)
    top = jnp.broadcast_to(jnp.max(s, axis=-1, keepdims=True), (query.shape[0], HEAD))
    new = top if m is None else jnp.maximum(m, top)
    p = jnp.exp2(s - jnp.concatenate([new] * (keys.shape[0] // HEAD), axis=1)).astype(bf16)
    add = dot(p, values)
    if m is not None:
        factor = jnp.exp2(m - new)
        add = acc * jnp.concatenate([factor, factor], axis=1) + add
    return new, add


def attend_body(tile, parts, first, *refs):
    q = refs[0]
    kvs = refs[1 : 1 + sum(parts)]
    rest = refs[1 + sum(parts) :]
    if first:
        w, lw, m_out, acc_out, w_v, lw_v, sems = rest
        copies = start_copies([(w, w_v), (lw, lw_v)], sems)
    else:
        m_out, acc_out = rest[-2:]
    for start in range(0, q.shape[0], tile):
        rows = pl.ds(start, tile)
        m, acc = (None, None) if first else (rest[0][rows, :], rest[1][rows, :])
        used = 0
        for count in parts:
            m, acc = softmax_step(q[rows, :], kvs[used : used + count], m, acc)
            used += count
        m_out[rows, :] = m
        acc_out[rows, :] = acc
    if first:
        for copy in copies:
            copy.wait()


def finish_body(flips, row_count, q, kv, m_in, acc_in, keep, send):
    _, core, pieces = place()
    piece = keep.shape[0] // len(flips)
    for i, flip in enumerate(flips):
        out_rows = pl.ds(i * piece, piece)
        for h in range(q.shape[0] // row_count):
            start = h * row_count + (pieces[3] ^ flip) * 2 * piece
            rows = pl.ds(pl.multiple_of(start, 16), 2 * piece)
            _, acc = softmax_step(q[rows, :], (kv,), m_in[rows, :], acc_in[rows, :])
            o = acc[:, :HEAD] / acc[:, HEAD:]
            lanes = slice(h * HEAD, (h + 1) * HEAD)
            keep[out_rows, lanes] = jnp.where(core == 0, o[:piece], o[piece:]).astype(bf16)
            send[out_rows, lanes] = jnp.where(core == 0, o[piece:], o[:piece]).astype(bf16)


def early_body(keep, lkeep, lother, w, lw, lw_other, out):
    piece = keep.shape[0]
    lrows = pl.ds(pl.multiple_of(place()[2][0] * piece, 16), piece)
    part = jnp.concatenate([keep[...], lkeep[lrows, :], lother[lrows, :]], axis=1)
    out[...] = dot(part, jnp.concatenate([w[...], lw[...], lw_other[...]], axis=0))


def pass_body(early, other, w_other, out):
    out[...] = (early[...] + dot(other[...], w_other[...])).astype(out.dtype)


def project_body(slots, keep, other, lkeep, lother, w, lw, w_other, lw_other, *outs):
    piece = outs[0].shape[-2]
    _, core, pieces = place()
    held = (0, core, 1 - core, 2)
    weights = jnp.concatenate([w[...], w_other[...], lw[...], lw_other[...]], axis=0)
    for slot, out in zip(slots, outs):
        rows = pl.ds(pl.multiple_of(held[slot] * piece, 16), piece)
        lrows = pl.ds(pl.multiple_of(pieces[slot] * piece, 16), piece)
        part = jnp.concatenate([keep[rows, :], other[rows, :], lkeep[lrows, :], lother[lrows, :]], axis=1)
        out[...] = dot(part, weights).astype(out.dtype)


def vmem(count):
    return [pl.BlockSpec(memory_space=pltpu.VMEM)] * count


def sds(shape, dtype):
    return jax.ShapeDtypeStruct(shape, dtype)


def cost(flops, transcendentals=0, bytes_accessed=0):
    return pl.CostEstimate(flops=int(COST * flops), transcendentals=int(transcendentals), bytes_accessed=int(bytes_accessed))


def hbm(count):
    return [pl.BlockSpec(memory_space=pltpu.HBM)] * count


def in_hbm(*arrays):
    return [pltpu.with_memory_space_constraint(a, pltpu.HBM) for a in arrays]


def params(mib):
    return pltpu.CompilerParams(vmem_limit_bytes=mib * MIB)


def attend(q, blocks, state, bring=()):
    rows = q.shape[0]
    operands = [q] + [part for block in blocks for part in block] + list(state or ())
    keys = sum(part.shape[0] for block in blocks for part in block)
    out_shape = (sds((rows, HEAD), f32), sds((rows, 2 * HEAD), f32)) + tuple(sds(a.shape, a.dtype) for a in bring)
    return pl.pallas_call(
        functools.partial(attend_body, 256, tuple(len(block) for block in blocks), state is None),
        out_shape=out_shape,
        in_specs=vmem(len(operands)) + hbm(len(bring)),
        out_specs=tuple(vmem(len(out_shape))),
        scratch_shapes=[pltpu.SemaphoreType.DMA((len(bring),))] if bring else [],
        compiler_params=params(16),
        cost_estimate=cost(rows * keys * HEAD * 8, rows * keys),
    )(*operands, *in_hbm(*bring))


def finish(q, kv, state, flips, row_count, piece):
    rows = q.shape[0]
    keys = kv.shape[0]
    done = 2 * piece * len(flips) * rows // row_count
    return pl.pallas_call(
        functools.partial(finish_body, flips, row_count),
        out_shape=(sds((piece * len(flips), rows // row_count * HEAD), bf16),) * 2,
        in_specs=vmem(4),
        out_specs=tuple(vmem(2)),
        compiler_params=params(16),
        cost_estimate=cost(done * keys * HEAD * 8, done * keys),
    )(q, kv, *state)


def project(slots, operands, piece, dtype):
    width = operands[-1].shape[1]
    depth = 4 * operands[0].shape[1]
    return pl.pallas_call(
        functools.partial(project_body, slots),
        out_shape=tuple(sds((piece, width), dtype) for _ in slots),
        in_specs=vmem(8),
        out_specs=tuple(vmem(len(slots))),
        compiler_params=params(8),
        cost_estimate=cost(2 * piece * width * depth * len(slots), 0, 4 * MIB),
    )(*operands)


def shards(
    tokens,
    norm_gain,
    grid_query_weight,
    grid_key_weight,
    grid_value_weight,
    grid_query_gain,
    grid_key_gain,
    local_query_weight,
    local_key_weight,
    local_value_weight,
    sink_logit,
    grid_out_weight,
    local_out_weight,
):
    row_count, width = tokens.shape
    n_sp = lax.axis_size("sp")
    n_tp = lax.axis_size("tp")
    total_rows = row_count * n_sp
    heads = grid_query_weight.shape[1] // HEAD
    row_np, col_np = turn_tables(total_rows, n_sp)
    row_tab, col_tab = jnp.asarray(row_np), jnp.asarray(col_np)

    tile = 128
    half = row_count // 2
    table_shape = (3, row_count // GRID_W, HEAD)

    tables = (sds((1, width), f32), sds((1, HEAD), f32), sds(table_shape, f32), sds((3, GRID_W, HEAD), f32))
    key_weights = grid_key_weight, grid_value_weight
    query_weights = grid_query_weight, local_query_weight, local_key_weight, local_value_weight
    rows_out = sds((half, width), bf16), sds((half, 2 * HEAD), bf16)
    key_cost = cost(2 * half * width * 2 * HEAD, 0, 4 * MIB)
    normed_a, kva, tokens_b, *shared = pl.pallas_call(
        functools.partial(first_keys_body, tile),
        out_shape=rows_out + (sds((half, width), bf16),) + tables + tuple(sds(w.shape, bf16) for w in key_weights),
        in_specs=hbm(7),
        out_specs=tuple(vmem(9)),
        scratch_shapes=[pltpu.VMEM((half, width), bf16), pltpu.SemaphoreType.DMA((7 + half // tile,))],
        compiler_params=params(16),
        cost_estimate=key_cost,
        name="keys_a",
    )(*in_hbm(tokens, norm_gain.reshape(1, width), grid_key_gain.reshape(1, HEAD), row_tab, col_tab, *key_weights))
    normed_b, kvb, *held = pl.pallas_call(
        second_keys_body,
        out_shape=rows_out + tuple(sds(w.shape, bf16) for w in query_weights) + (sds((1, HEAD), f32),),
        in_specs=vmem(7) + hbm(5),
        out_specs=tuple(vmem(7)),
        scratch_shapes=[pltpu.SemaphoreType.DMA((5,))],
        compiler_params=params(16),
        cost_estimate=key_cost,
        name="keys_b",
    )(tokens_b, *shared, *in_hbm(*query_weights, grid_query_gain.reshape(1, HEAD)))

    forward = [(i, (i + 1) % n_sp) for i in range(n_sp)]
    backward = [(t, s) for s, t in forward]


    def shift(low, high):
        low_a = lax.ppermute(low[0], "sp", forward)
        high_a = lax.ppermute(high[0], "sp", backward)
        low_b = lax.ppermute(low[1], "sp", forward)
        high_b = lax.ppermute(high[1], "sp", backward)
        return (low_a, low_b), (high_a, high_b)

    low, high = shift((kva, kvb), (kva, kvb))

    q, lq, lkv, first_edge, last_edge = pl.pallas_call(
        q_body,
        out_shape=(
            sds((heads * row_count, HEAD), bf16),
            sds((row_count, heads * HEAD), bf16),
            sds((row_count, 2 * HEAD), bf16),
            sds((WINDOW, 2 * HEAD), bf16),
            sds((WINDOW, 2 * HEAD), bf16),
        ),
        in_specs=vmem(9),
        out_specs=tuple(vmem(5)),
        compiler_params=params(16),
        cost_estimate=cost(2 * row_count * width * 6 * HEAD, 0, 6 * MIB),
        name="queries",
    )(normed_a, normed_b, *held, *shared[2:4])

    flip = [(i, i ^ 1) for i in range(n_tp)]
    first_hop = [(i, i ^ (2 + 2 * (i % 2))) for i in range(n_tp)]
    second_hop = [(i, i ^ (4 - 2 * (i % 2))) for i in range(n_tp)]
    low_edge = lax.ppermute(last_edge, "sp", forward[:-1])
    high_edge = lax.ppermute(first_edge, "sp", backward[:-1])
    *state, w_own, lw_own = attend(q, [(kva, kvb), (low[0], high[0])], None, (grid_out_weight, local_out_weight))
    w_other = lax.ppermute(w_own, "tp", flip)
    lw_other = lax.ppermute(lw_own, "tp", flip)
    for _ in range(1, (n_sp - 1) // 2):
        next_low, next_high = shift(low, high)
        state = attend(q, [(low[1], high[1]), (next_low[0], next_high[0])], state)
        low, high = next_low, next_high
    far = lax.ppermute(low[0], "sp", forward), lax.ppermute(high[1], "sp", backward)

    lkeep, lsend = pl.pallas_call(
        functools.partial(local_body, row_count // WINDOW, total_rows),
        out_shape=(sds((row_count // 2, heads * HEAD), bf16),) * 2,
        in_specs=vmem(5),
        out_specs=tuple(vmem(2)),
        scratch_shapes=[pltpu.VMEM((row_count, heads * HEAD), bf16)],
        compiler_params=params(16),
        cost_estimate=cost(heads * row_count * 3 * WINDOW * HEAD * 8, heads * row_count * 3 * WINDOW),
        name="banded",
    )(sink_logit.reshape(1, heads), lq, lkv, low_edge, high_edge)
    lother = lax.ppermute(lsend, "tp", flip)
    state = attend(q, [(low[1], high[1])], state)

    piece = row_count // n_tp
    state = attend(q, [(far[0],)], state)
    keep, send = finish(q, far[1], state, (3,), row_count, piece)
    other = lax.ppermute(send, "tp", flip)
    keep_rest, send_rest = finish(q, far[1], state, (1, 2, 0), row_count, piece)
    other_rest = lax.ppermute(send_rest, "tp", flip)

    fixed = (lkeep, lother, w_own, lw_own, w_other, lw_other)
    early = pl.pallas_call(
        early_body,
        out_shape=sds((piece, width), f32),
        in_specs=vmem(6),
        out_specs=vmem(1)[0],
        compiler_params=params(8),
        cost_estimate=cost(6 * piece * width * heads * HEAD),
        name="early",
    )(keep, lkeep, lother, w_own, lw_own, lw_other)
    pass_on = pl.pallas_call(
        pass_body,
        out_shape=sds((piece, width), bf16),
        in_specs=vmem(3),
        out_specs=vmem(1)[0],
        compiler_params=params(8),
        cost_estimate=cost(2 * piece * width * heads * HEAD),
        name="pass_on",
    )(early, other, w_other)
    got_on = lax.ppermute(pass_on, "tp", first_hop)
    next_part, own_part = project((2, 3), (keep_rest, other_rest) + fixed, piece, f32)
    (direct,) = project((1,), (keep_rest, other_rest) + fixed, piece, bf16)
    got = lax.ppermute(direct, "tp", first_hop)
    got_next = lax.ppermute((next_part + got_on.astype(f32)).astype(bf16), "tp", second_hop)
    summed = lax.optimization_barrier(own_part + got.astype(f32))
    return (summed + got_next.astype(f32)).astype(bf16)


def solution(mesh):
    in_specs = (
        P("sp", None),
        P(),
        P(None, "tp"),
        P(None, "tp"),
        P(None, "tp"),
        P(),
        P(),
        P(None, "tp"),
        P(None, "tp"),
        P(None, "tp"),
        P("tp"),
        P("tp", None),
        P("tp", None),
    )
    out_specs = P(("sp", "tp"), None)

    return jax.shard_map(shards, mesh=mesh, in_specs=in_specs, out_specs=out_specs, check_vma=False)
```

```python
import functools
import math

import jax
import jax.numpy as jnp
import numpy as np
from jax import lax
from jax.experimental import pallas as pl
from jax.experimental.pallas import tpu as pltpu
from jax.sharding import PartitionSpec as P


HEAD = 128
WINDOW = 128
GRID_W = 64
EPSILON = 1e-06
ROPE_BASE = 10000.0
MASKED = -1e30
LOG2E = math.log2(math.e)
MIB = 1 << 20
COST = 0.3

bf16 = jnp.bfloat16
f32 = jnp.float32
ROWS_T = (((1,), (1,)), ((), ()))


def dot(a, b):
    return jnp.dot(a, b, preferred_element_type=f32)


def turn_tables(total_rows, seq_devices):
    half = HEAD // 2
    quarter = half // 2
    inverse = (ROPE_BASE ** (-np.arange(0, half, 2, dtype=np.float32) / np.float32(half))).astype(np.float32)

    def tables(count, first):
        angles = np.arange(count, dtype=np.float32)[:, None] * inverse
        out = np.zeros((3, count, HEAD), np.float32)
        base = 0 if first else half
        out[0, :, base : base + quarter] = np.cos(angles)
        out[0, :, base + quarter : base + half] = np.cos(angles)
        out[1, :, base : base + quarter] = -np.sin(angles)
        out[2, :, base + quarter : base + half] = np.sin(angles)
        return out

    rows = tables(total_rows // GRID_W, True)
    rows = rows.reshape(3, seq_devices, -1, HEAD).transpose(1, 0, 2, 3)
    return rows, tables(GRID_W, False)


def norm_turn(part, gain, row_tab, col_tab, first_row, grid_rows):
    x = part.astype(bf16).astype(f32)
    x = x * lax.rsqrt(jnp.mean(x * x, axis=-1, keepdims=True) + EPSILON) * gain

    def table(k):
        rows = row_tab[k, pl.ds(first_row, grid_rows), :]
        return (rows[:, None, :] + col_tab[k][None, :, :]).reshape(grid_rows * GRID_W, HEAD)

    quarter = HEAD // 4
    return (
        x * table(0)
        + pltpu.roll(x, HEAD - quarter, 1) * table(1)
        + pltpu.roll(x, quarter, 1) * table(2)
    )


def place():
    tp = lax.axis_index("tp")
    core, mine = tp % 2, tp // 2
    return lax.axis_index("sp"), core, (mine ^ 3, mine ^ (1 + core), mine ^ (2 - core), mine)


def start_copies(pairs, sems):
    copies = [pltpu.make_async_copy(src, dst, sems.at[i]) for i, (src, dst) in enumerate(pairs)]
    for copy in copies:
        copy.start()
    return copies


def norm_rows(x, gain):
    x = x.astype(f32)
    return (x * lax.rsqrt(jnp.mean(x * x, axis=-1, keepdims=True) + EPSILON) * gain).astype(bf16)


def kv_rows(first_row, normed, wk, wv, kgain, row_tab, col_tab, kv):
    y = dot(normed[...], jnp.concatenate([wk[...], wv[...]], axis=1))
    keys = norm_turn(y[:, :HEAD], kgain[...], row_tab, col_tab, first_row // GRID_W, normed.shape[0] // GRID_W)
    kv[...] = jnp.concatenate([keys, y[:, HEAD:]], axis=1).astype(bf16)


def first_keys_body(tile, tok, gain, kgain, row_tab, col_tab, wk, wv,
                    normed, kv, gain_v, kgain_v, row_v, col_v, wk_v, wv_v, tok_v, sems):
    half = normed.shape[0]
    rows = [pl.ds(i, tile) for i in range(0, half, tile)]
    pairs = [(gain, gain_v)] + [(tok.at[r], tok_v.at[r]) for r in rows] + [(wk, wk_v), (wv, wv_v)]
    pairs += [(kgain, kgain_v), (row_tab.at[place()[0]], row_v), (col_tab, col_v)]
    copies = start_copies(pairs, sems)
    copies[0].wait()
    for r, copy in zip(rows, copies[1:]):
        copy.wait()
        normed[r, :] = norm_rows(tok_v[r, :], gain_v[...])
    for copy in copies[1 + len(rows) :]:
        copy.wait()
    kv_rows(0, normed, wk_v, wv_v, kgain_v, row_v, col_v, kv)


def second_keys_body(tile, gain, kgain, row_tab, col_tab, wk, wv, tok, wq, lwq, lwk, lwv, qgain,
                     normed, kv, wq_v, lwq_v, lwk_v, lwv_v, qgain_v, tok_v, sems):
    half = normed.shape[0]
    rows = [pl.ds(i, tile) for i in range(0, half, tile)]
    pairs = [(tok.at[pl.ds(half + r.start, tile)], tok_v.at[r]) for r in rows]
    pairs += [(wq, wq_v), (lwq, lwq_v), (lwk, lwk_v), (lwv, lwv_v), (qgain, qgain_v)]
    copies = start_copies(pairs, sems)
    for r, copy in zip(rows, copies):
        copy.wait()
        normed[r, :] = norm_rows(tok_v[r, :], gain[...])
    kv_rows(half, normed, wk, wv, kgain, row_tab, col_tab, kv)
    for copy in copies[len(rows) :]:
        copy.wait()


def q_body(normed_a, normed_b, wq, lwq, lwk, lwv, qgain, row_tab, col_tab, q, lq, lkv, first_edge, last_edge):
    row_count = lq.shape[0]
    tile = row_count // 2
    heads = wq.shape[1] // HEAD
    gain = qgain[...] * (HEAD ** (-0.5) * LOG2E)
    for start, normed in ((0, normed_a), (tile, normed_b)):
        rows = pl.ds(start, tile)
        y = dot(normed[...], jnp.concatenate([wq[...], lwq[...], lwk[...], lwv[...]], axis=1))
        for h in range(heads):
            part = y[:, h * HEAD : (h + 1) * HEAD]
            turned = norm_turn(part, gain, row_tab, col_tab, start // GRID_W, tile // GRID_W)
            q[pl.ds(h * row_count + start, tile), :] = turned.astype(bf16)
        lq[rows, :] = y[:, heads * HEAD : 2 * heads * HEAD].astype(bf16)
        lkv[rows, :] = y[:, 2 * heads * HEAD :].astype(bf16)
    first_edge[...] = lkv[pl.ds(0, WINDOW), :]
    last_edge[...] = lkv[pl.ds(row_count - WINDOW, WINDOW), :]


def split_rows(whole, keep, send):
    piece = keep.shape[0] // (whole.shape[0] // keep.shape[0] * 2)
    count = keep.shape[0] // piece
    core = place()[1]
    for part, flip in ((keep, 0), (send, 1)):
        for i in range(count):
            start = pl.multiple_of(2 * i * piece + (core ^ flip) * piece, 16)
            part[pl.ds(i * piece, piece), :] = whole[pl.ds(start, piece), :]


def local_body(blocks, total_rows, sink, lq, lkv, low, high, keep, send, out):
    offset = place()[0] * (blocks * WINDOW)
    scale = HEAD ** (-0.5) * LOG2E
    heads = lq.shape[1] // HEAD
    shape = (heads * WINDOW, 3 * WINDOW)
    row = lax.broadcasted_iota(jnp.int32, shape, 0) % WINDOW
    col = lax.broadcasted_iota(jnp.int32, shape, 1)
    band = jnp.abs(col - WINDOW - row) <= WINDOW
    bound = jnp.concatenate(
        [jnp.broadcast_to(sink[:, h : h + 1] * LOG2E, (WINDOW, 1)) for h in range(heads)], axis=0
    )
    ones = jnp.ones((3 * WINDOW, HEAD), bf16)
    pieces = [low[...]] + [lkv[pl.ds(i * WINDOW, WINDOW), :] for i in range(blocks)] + [high[...]]
    for i in range(blocks):
        keys = jnp.concatenate([p[:, :HEAD] for p in pieces[i : i + 3]], axis=0)
        values = jnp.concatenate([p[:, HEAD:] for p in pieces[i : i + 3]], axis=0)
        valid = band
        if i == 0 or i == blocks - 1:
            pos = offset + (i - 1) * WINDOW + col
            valid = band & (pos >= 0) & (pos < total_rows)
        rows = pl.ds(i * WINDOW, WINDOW)
        query = jnp.concatenate([lq[rows, h * HEAD : (h + 1) * HEAD] for h in range(heads)], axis=0)
        s = lax.dot_general(query, keys, ROWS_T, preferred_element_type=f32) * scale
        s = jnp.where(valid, s, MASKED)
        top = jnp.maximum(jnp.max(s, axis=-1, keepdims=True), bound)
        p = jnp.exp2(s - top).astype(bf16)
        o = dot(p, jnp.concatenate([values, ones], axis=1))
        o = (o[:, :HEAD] / (o[:, HEAD:] + jnp.exp2(bound - top))).astype(bf16)
        for h in range(heads):
            out[rows, h * HEAD : (h + 1) * HEAD] = o[h * WINDOW : (h + 1) * WINDOW]
    split_rows(out, keep, send)


def softmax_step(query, pairs, m, acc):
    keys = jnp.concatenate([kv[:, :HEAD] for kv in pairs], axis=0)
    values = jnp.concatenate([kv[:, HEAD:] for kv in pairs], axis=0)
    values = jnp.concatenate([values, jnp.ones_like(values)], axis=1)
    s = lax.dot_general(query, keys, ROWS_T, preferred_element_type=f32)
    top = jnp.broadcast_to(jnp.max(s, axis=-1, keepdims=True), (query.shape[0], HEAD))
    new = top if m is None else jnp.maximum(m, top)
    p = jnp.exp2(s - jnp.concatenate([new] * (keys.shape[0] // HEAD), axis=1)).astype(bf16)
    add = dot(p, values)
    if m is not None:
        factor = jnp.exp2(m - new)
        add = acc * jnp.concatenate([factor, factor], axis=1) + add
    return new, add


def attend_body(tile, parts, first, *refs):
    q = refs[0]
    kvs = refs[1 : 1 + sum(parts)]
    rest = refs[1 + sum(parts) :]
    if first:
        w, lw, m_out, acc_out, w_v, lw_v, sems = rest
        copies = start_copies([(w, w_v), (lw, lw_v)], sems)
    else:
        m_out, acc_out = rest[-2:]
    for start in range(0, q.shape[0], tile):
        rows = pl.ds(start, tile)
        m, acc = (None, None) if first else (rest[0][rows, :], rest[1][rows, :])
        used = 0
        for count in parts:
            m, acc = softmax_step(q[rows, :], kvs[used : used + count], m, acc)
            used += count
        m_out[rows, :] = m
        acc_out[rows, :] = acc
    if first:
        for copy in copies:
            copy.wait()


def finish_body(flips, row_count, q, kv, m_in, acc_in, keep, send):
    _, core, pieces = place()
    piece = keep.shape[0] // len(flips)
    for i, flip in enumerate(flips):
        out_rows = pl.ds(i * piece, piece)
        for h in range(q.shape[0] // row_count):
            start = h * row_count + (pieces[3] ^ flip) * 2 * piece
            rows = pl.ds(pl.multiple_of(start, 16), 2 * piece)
            _, acc = softmax_step(q[rows, :], (kv,), m_in[rows, :], acc_in[rows, :])
            o = acc[:, :HEAD] / acc[:, HEAD:]
            lanes = slice(h * HEAD, (h + 1) * HEAD)
            keep[out_rows, lanes] = jnp.where(core == 0, o[:piece], o[piece:]).astype(bf16)
            send[out_rows, lanes] = jnp.where(core == 0, o[piece:], o[:piece]).astype(bf16)


def early_body(keep, lkeep, lother, w, lw, lw_other, out):
    piece = keep.shape[0]
    lrows = pl.ds(pl.multiple_of(place()[2][0] * piece, 16), piece)
    part = jnp.concatenate([keep[...], lkeep[lrows, :], lother[lrows, :]], axis=1)
    out[...] = dot(part, jnp.concatenate([w[...], lw[...], lw_other[...]], axis=0))


def pass_body(early, other, w_other, out):
    out[...] = (early[...] + dot(other[...], w_other[...])).astype(out.dtype)


def project_body(slots, keep, other, lkeep, lother, w, lw, w_other, lw_other, *outs):
    piece = outs[0].shape[-2]
    _, core, pieces = place()
    held = (0, core, 1 - core, 2)
    weights = jnp.concatenate([w[...], w_other[...], lw[...], lw_other[...]], axis=0)
    for slot, out in zip(slots, outs):
        rows = pl.ds(pl.multiple_of(held[slot] * piece, 16), piece)
        lrows = pl.ds(pl.multiple_of(pieces[slot] * piece, 16), piece)
        part = jnp.concatenate([keep[rows, :], other[rows, :], lkeep[lrows, :], lother[lrows, :]], axis=1)
        out[...] = dot(part, weights).astype(out.dtype)


def vmem(count):
    return [pl.BlockSpec(memory_space=pltpu.VMEM)] * count


def sds(shape, dtype):
    return jax.ShapeDtypeStruct(shape, dtype)


def cost(flops, transcendentals=0, bytes_accessed=0):
    return pl.CostEstimate(flops=int(COST * flops), transcendentals=int(transcendentals), bytes_accessed=int(bytes_accessed))


def hbm(count):
    return [pl.BlockSpec(memory_space=pltpu.HBM)] * count


def in_hbm(*arrays):
    return [pltpu.with_memory_space_constraint(a, pltpu.HBM) for a in arrays]


def params(mib):
    return pltpu.CompilerParams(vmem_limit_bytes=mib * MIB)


def attend(q, blocks, state, bring=()):
    rows = q.shape[0]
    operands = [q] + [part for block in blocks for part in block] + list(state or ())
    keys = sum(part.shape[0] for block in blocks for part in block)
    out_shape = (sds((rows, HEAD), f32), sds((rows, 2 * HEAD), f32)) + tuple(sds(a.shape, a.dtype) for a in bring)
    return pl.pallas_call(
        functools.partial(attend_body, 256, tuple(len(block) for block in blocks), state is None),
        out_shape=out_shape,
        in_specs=vmem(len(operands)) + hbm(len(bring)),
        out_specs=tuple(vmem(len(out_shape))),
        scratch_shapes=[pltpu.SemaphoreType.DMA((len(bring),))] if bring else [],
        compiler_params=params(16),
        cost_estimate=cost(rows * keys * HEAD * 8, rows * keys),
    )(*operands, *in_hbm(*bring))


def finish(q, kv, state, flips, row_count, piece):
    rows = q.shape[0]
    keys = kv.shape[0]
    done = 2 * piece * len(flips) * rows // row_count
    return pl.pallas_call(
        functools.partial(finish_body, flips, row_count),
        out_shape=(sds((piece * len(flips), rows // row_count * HEAD), bf16),) * 2,
        in_specs=vmem(4),
        out_specs=tuple(vmem(2)),
        compiler_params=params(16),
        cost_estimate=cost(done * keys * HEAD * 8, done * keys),
    )(q, kv, *state)


def project(slots, operands, piece, dtype):
    width = operands[-1].shape[1]
    depth = 4 * operands[0].shape[1]
    return pl.pallas_call(
        functools.partial(project_body, slots),
        out_shape=tuple(sds((piece, width), dtype) for _ in slots),
        in_specs=vmem(8),
        out_specs=tuple(vmem(len(slots))),
        compiler_params=params(8),
        cost_estimate=cost(2 * piece * width * depth * len(slots), 0, 4 * MIB),
    )(*operands)


def shards(
    tokens,
    norm_gain,
    grid_query_weight,
    grid_key_weight,
    grid_value_weight,
    grid_query_gain,
    grid_key_gain,
    local_query_weight,
    local_key_weight,
    local_value_weight,
    sink_logit,
    grid_out_weight,
    local_out_weight,
):
    row_count, width = tokens.shape
    n_sp = lax.axis_size("sp")
    n_tp = lax.axis_size("tp")
    total_rows = row_count * n_sp
    heads = grid_query_weight.shape[1] // HEAD
    row_np, col_np = turn_tables(total_rows, n_sp)
    row_tab, col_tab = jnp.asarray(row_np), jnp.asarray(col_np)

    tile = 128
    half = row_count // 2
    table_shape = (3, row_count // GRID_W, HEAD)

    tables = (sds((1, width), f32), sds((1, HEAD), f32), sds(table_shape, f32), sds((3, GRID_W, HEAD), f32))
    key_weights = grid_key_weight, grid_value_weight
    query_weights = grid_query_weight, local_query_weight, local_key_weight, local_value_weight
    rows_out = sds((half, width), bf16), sds((half, 2 * HEAD), bf16)
    key_cost = cost(2 * half * width * 2 * HEAD, 0, 4 * MIB)
    normed_a, kva, *shared = pl.pallas_call(
        functools.partial(first_keys_body, tile),
        out_shape=rows_out + tables + tuple(sds(w.shape, bf16) for w in key_weights),
        in_specs=hbm(7),
        out_specs=tuple(vmem(8)),
        scratch_shapes=[pltpu.VMEM((half, width), bf16), pltpu.SemaphoreType.DMA((6 + half // tile,))],
        compiler_params=params(16),
        cost_estimate=key_cost,
        name="keys_a",
    )(*in_hbm(tokens, norm_gain.reshape(1, width), grid_key_gain.reshape(1, HEAD), row_tab, col_tab, *key_weights))
    normed_b, kvb, *held = pl.pallas_call(
        functools.partial(second_keys_body, tile),
        out_shape=rows_out + tuple(sds(w.shape, bf16) for w in query_weights) + (sds((1, HEAD), f32),),
        in_specs=vmem(6) + hbm(6),
        out_specs=tuple(vmem(7)),
        scratch_shapes=[pltpu.VMEM((half, width), bf16), pltpu.SemaphoreType.DMA((5 + half // tile,))],
        compiler_params=params(16),
        cost_estimate=key_cost,
        name="keys_b",
    )(*shared, *in_hbm(tokens, *query_weights, grid_query_gain.reshape(1, HEAD)))

    forward = [(i, (i + 1) % n_sp) for i in range(n_sp)]
    backward = [(t, s) for s, t in forward]


    def shift(low, high):
        low_a = lax.ppermute(low[0], "sp", forward)
        high_a = lax.ppermute(high[0], "sp", backward)
        low_b = lax.ppermute(low[1], "sp", forward)
        high_b = lax.ppermute(high[1], "sp", backward)
        return (low_a, low_b), (high_a, high_b)

    low, high = shift((kva, kvb), (kva, kvb))

    q, lq, lkv, first_edge, last_edge = pl.pallas_call(
        q_body,
        out_shape=(
            sds((heads * row_count, HEAD), bf16),
            sds((row_count, heads * HEAD), bf16),
            sds((row_count, 2 * HEAD), bf16),
            sds((WINDOW, 2 * HEAD), bf16),
            sds((WINDOW, 2 * HEAD), bf16),
        ),
        in_specs=vmem(9),
        out_specs=tuple(vmem(5)),
        compiler_params=params(16),
        cost_estimate=cost(2 * row_count * width * 6 * HEAD, 0, 6 * MIB),
        name="queries",
    )(normed_a, normed_b, *held, *shared[2:4])

    flip = [(i, i ^ 1) for i in range(n_tp)]
    first_hop = [(i, i ^ (2 + 2 * (i % 2))) for i in range(n_tp)]
    second_hop = [(i, i ^ (4 - 2 * (i % 2))) for i in range(n_tp)]
    low_edge = lax.ppermute(last_edge, "sp", forward[:-1])
    high_edge = lax.ppermute(first_edge, "sp", backward[:-1])
    *state, w_own, lw_own = attend(q, [(kva, kvb), (low[0], high[0])], None, (grid_out_weight, local_out_weight))
    w_other = lax.ppermute(w_own, "tp", flip)
    lw_other = lax.ppermute(lw_own, "tp", flip)
    for _ in range(1, (n_sp - 1) // 2):
        next_low, next_high = shift(low, high)
        state = attend(q, [(low[1], high[1]), (next_low[0], next_high[0])], state)
        low, high = next_low, next_high
    far = lax.ppermute(low[0], "sp", forward), lax.ppermute(high[1], "sp", backward)

    lkeep, lsend = pl.pallas_call(
        functools.partial(local_body, row_count // WINDOW, total_rows),
        out_shape=(sds((row_count // 2, heads * HEAD), bf16),) * 2,
        in_specs=vmem(5),
        out_specs=tuple(vmem(2)),
        scratch_shapes=[pltpu.VMEM((row_count, heads * HEAD), bf16)],
        compiler_params=params(16),
        cost_estimate=cost(heads * row_count * 3 * WINDOW * HEAD * 8, heads * row_count * 3 * WINDOW),
        name="banded",
    )(sink_logit.reshape(1, heads), lq, lkv, low_edge, high_edge)
    lother = lax.ppermute(lsend, "tp", flip)
    state = attend(q, [(low[1], high[1])], state)

    piece = row_count // n_tp
    state = attend(q, [(far[0],)], state)
    keep, send = finish(q, far[1], state, (3,), row_count, piece)
    other = lax.ppermute(send, "tp", flip)
    keep_rest, send_rest = finish(q, far[1], state, (1, 2, 0), row_count, piece)
    other_rest = lax.ppermute(send_rest, "tp", flip)

    fixed = (lkeep, lother, w_own, lw_own, w_other, lw_other)
    early = pl.pallas_call(
        early_body,
        out_shape=sds((piece, width), f32),
        in_specs=vmem(6),
        out_specs=vmem(1)[0],
        compiler_params=params(8),
        cost_estimate=cost(6 * piece * width * heads * HEAD),
        name="early",
    )(keep, lkeep, lother, w_own, lw_own, lw_other)
    pass_on = pl.pallas_call(
        pass_body,
        out_shape=sds((piece, width), bf16),
        in_specs=vmem(3),
        out_specs=vmem(1)[0],
        compiler_params=params(8),
        cost_estimate=cost(2 * piece * width * heads * HEAD),
        name="pass_on",
    )(early, other, w_other)
    got_on = lax.ppermute(pass_on, "tp", first_hop)
    next_part, own_part = project((2, 3), (keep_rest, other_rest) + fixed, piece, f32)
    (direct,) = project((1,), (keep_rest, other_rest) + fixed, piece, bf16)
    got = lax.ppermute(direct, "tp", first_hop)
    got_next = lax.ppermute((next_part + got_on.astype(f32)).astype(bf16), "tp", second_hop)
    summed = own_part + got.astype(f32)
    return (summed + got_next.astype(f32)).astype(bf16)


def solution(mesh):
    in_specs = (
        P("sp", None),
        P(),
        P(None, "tp"),
        P(None, "tp"),
        P(None, "tp"),
        P(),
        P(),
        P(None, "tp"),
        P(None, "tp"),
        P(None, "tp"),
        P("tp"),
        P("tp", None),
        P("tp", None),
    )
    out_specs = P(("sp", "tp"), None)

    return jax.shard_map(shards, mesh=mesh, in_specs=in_specs, out_specs=out_specs, check_vma=False)
```
